32 devices in a mesh: ep: 8 (over z, x), tp: 4 (over y, core).
Axes of the slice: x: 2, y: 2, z: 4, core: 2. Of those that a mesh axis runs over, the one named last changes fastest.
Arguments:
- query_rows: bfloat16 [3072, 1024], P('ep', 'tp'), may hold values from -8 to 8
- key_rows: bfloat16 [3072, 256], P('ep'), may hold values from -8 to 8
- value_rows: bfloat16 [3072, 256], P('ep'), may hold values from -6 to 6
- query_gain: float32 [64], replicated, may hold values from 0.3 to 6
- key_gain: float32 [64], replicated, may hold values from 0.3 to 6
- out_weight: bfloat16 [1024, 2048], P('tp'), may hold values from -0.1875 to 0.1875
- mixer_gain: float32 [2048], replicated, may hold values from 0.1 to 1.9
- expert_input: bfloat16 [2048, 2048], P('ep'), may hold values from -6 to 6
- expert_ids: int32 [2048, 2], P('ep'), may hold values from 0 to 7, all different within a row; in each aligned block of 256 rows (0 to 255, 256 to 511, ...) at most 96 rows name the same one
- gate_score: float32 [2048, 2], P('ep'), may hold values from 0.05 to 1
- expert_gain: float32 [2048], replicated, may hold values from 0.1 to 1.9
- gate_weight: bfloat16 [8, 2048, 4096], P('ep', None, 'tp'), may hold values from -0.125 to 0.125
- up_weight: bfloat16 [8, 2048, 4096], P('ep', None, 'tp'), may hold values from -0.125 to 0.125
- down_weight: bfloat16 [8, 4096, 2048], P('ep', 'tp'), may hold values from -0.09375 to 0.09375
- shared_gate: bfloat16 [2048, 2048], P(None, 'tp'), may hold values from -0.125 to 0.125
- shared_up: bfloat16 [2048, 2048], P(None, 'tp'), may hold values from -0.125 to 0.125
- shared_down: bfloat16 [2048, 2048], P('tp'), may hold values from -0.125 to 0.125
Outputs:
- mixer_out: bfloat16 [3072, 2048], P('ep')
- expert_out: bfloat16 [2048, 2048], P('ep', 'tp')
The draws below stay inside these ranges and needn't reach their ends.
Inputs may be any that keep to these rules, and one draw needn't show every extreme that they name: `expert_ids`: each row names 2 different experts. In each aligned block of 256 rows (the rows of one device) no expert is named by more than 96 rows, a bound that some block reaches.
All inputs are finite; a program needn't handle non-finite values.
Results may differ from the reference program's by a relative error of at most 0.02.
The reference program's roundings to bfloat16 on the way count: a program that leaves them out, or rounds other values in their place, can miss the bound.
Values may be sent and summed in bfloat16 or wider, within the bound.
No kernel may reach another device: no remote copies, remote signals or barrier semaphores. Data moves between devices by JAX's collectives and lax.ppermute only.
A program may use at most 128 MiB of HBM per device.

```python
import math
import jax
import jax.numpy as jnp
import numpy as np
from jax import lax

D = 2048
HEADS = 16
KV_HEADS = 4
HEAD_DIM = 64
GRID_W = 64
EXPERT_DIM = 4096
SHARED_DIM = 2048
TOP = 2
RA = 384
RB = 256
TA = 3072
TB = 2048
EXPERTS = 8
CAP = 96
N_EP = 8
N_TP = 4


def draw_query_rows(key, part):
    drawn = jax.random.normal(jax.random.fold_in(key, 11), (TA, HEADS * HEAD_DIM), jnp.float32)
    drawn = jnp.clip(drawn, -6.0, 6.0)
    return drawn.astype(jnp.bfloat16)


def draw_key_rows(key, part):
    drawn = jax.random.normal(jax.random.fold_in(key, 12), (TA, KV_HEADS * HEAD_DIM), jnp.float32)
    drawn = jnp.clip(drawn, -6.0, 6.0)
    return drawn.astype(jnp.bfloat16)


def gain_draw(key, salt):
    drawn = 1.0 + 0.18 * jax.random.normal(jax.random.fold_in(key, salt), (HEAD_DIM,), jnp.float32)
    drawn = jnp.clip(drawn, 0.3, 1.7)
    return drawn.astype(jnp.float32)


def draw_query_gain(key, part):
    return gain_draw(key, 21)


def draw_key_gain(key, part):
    return gain_draw(key, 22)


def shard_levels(key, shape, cuts, low, top_value):
    level, own = 1.0, jax.random.fold_in(key, 6)
    for dim, parts in cuts:
        heights = jnp.exp(jax.random.uniform(jax.random.fold_in(own, dim), (parts,), jnp.float32, low / len(cuts), top_value / len(cuts)))
        level = level * jnp.repeat(heights, shape[dim] // parts).reshape([-1 if axis == dim else 1 for axis in range(len(shape))])
    return level


def assign_block(rng, own, number, rows, count, top, limit, lean):
    sequence = jax.random.permutation(rng, count)
    heavy_load, ordinary = load_shares(count, rows * top, limit, lean, True), load_shares(count, rows * top, limit, lean, False)
    places = jnp.arange(count)

    def named(tallies, rotation):
        used = int((tallies > 0).sum())
        fixed = max(1, used // 4)
        moved = fixed + (places - fixed + rotation * (used - fixed)) % max(1, count - fixed)
        return jnp.zeros((count,), jnp.int32).at[sequence[jnp.where(places < fixed, places, moved)]].set(jnp.asarray(tallies, jnp.int32))

    tallies = jnp.where(number % 4 == 0, named(heavy_load, number // 4), named(ordinary, number - number // 4 - 1))
    mixed = jax.random.permutation(jax.random.fold_in(own, 3), count)
    donor, taker = mixed[0:count // 2 * 2:2], mixed[1:count // 2 * 2:2]
    slack = jnp.minimum(tallies[donor] - 1, limit - tallies[taker]) // 2
    slack = jnp.where((donor == sequence[0]) | (taker == sequence[0]) | (tallies[taker] == 0), 0, jnp.maximum(slack, 0))
    moved = jax.random.randint(jax.random.fold_in(own, 4), (count // 2,), 0, 1 << 20) % (slack + 1)
    tallies = tallies.at[donor].add(-moved).at[taker].add(moved)
    items = jnp.searchsorted(jnp.cumsum(tallies), jnp.arange(rows * top), side="right").astype(jnp.int32)
    table = items.reshape(top, rows).T
    table = table[jax.random.permutation(jax.random.fold_in(own, 1), rows)]
    rotation = jax.random.randint(jax.random.fold_in(own, 2), (rows, 1), 0, top)
    return jnp.take_along_axis(table, (jnp.arange(top)[None, :] + rotation) % top, axis=1)


def load_shares(number_of, total, bound, lean, full):
    weights = [(1 << 20) // math.isqrt(standing ** lean) + 1 for standing in range(1, number_of + 1)]
    largest = bound if full else min(bound, max(-(-total // number_of), total * weights[0] // sum(weights)))
    least = 1 if total - largest >= number_of - 1 else 0
    holding, spare = [largest] + [least] * (number_of - 1), total - largest - least * (number_of - 1)
    while spare > 0:
        free = [i for i in range(1, number_of) if holding[i] < largest] or [i for i in range(1, number_of) if holding[i] < bound]
        pool, budget = sum([weights[i] for i in free]), spare
        for i in free:
            addition = min(bound - holding[i], max(1, budget * weights[i] // pool), spare)
            holding[i] = holding[i] + addition
            spare = spare - addition
    return np.array(holding)


def centred(own_key, extent, spread, most, pieces=(), kind=jnp.bfloat16):
    result = spread * jax.random.normal(own_key, extent, jnp.float32)
    if pieces:
        result = result * shard_levels(own_key, extent, pieces, -0.22, 0.18)
    return jnp.clip(result, -most, most).astype(kind)


def setup_inputs(seed: int = 0) -> dict:
    key_of = jax.random.split(jax.random.key(seed), 18)
    query_rows = draw_query_rows(jax.random.fold_in(key_of[17], 71), 0)
    key_rows = draw_key_rows(jax.random.fold_in(key_of[17], 71), 0)
    value_rows = centred(key_of[2], (TA, KV_HEADS * HEAD_DIM), 1.0, 6.0, ((0, 8),))
    query_gain = draw_query_gain(jax.random.fold_in(key_of[17], 71), 0)
    key_gain = draw_key_gain(jax.random.fold_in(key_of[17], 71), 0)
    out_weight = centred(key_of[5], (HEADS * HEAD_DIM, D), (HEADS * HEAD_DIM) ** -0.5, 0.1875, ((0, 4),))
    mixer_gain = jnp.clip(1.0 + 0.18 * jax.random.normal(key_of[6], (D,), jnp.float32), 0.1, 1.9)
    expert_input = centred(key_of[7], (TB, D), 1.0, 6.0, ((0, 8),))
    expert_ids_keys = jax.random.split(jax.random.fold_in(key_of[8], 1), TB // RB)
    expert_ids_turns = jax.random.permutation(jax.random.fold_in(key_of[8], 3), TB // RB)
    expert_ids = jax.vmap(lambda own, number: assign_block(jax.random.fold_in(key_of[8], 2), own, number, RB, EXPERTS, TOP, CAP, 2))(expert_ids_keys, expert_ids_turns).reshape((TB, TOP))
    gate_score = jnp.clip(jnp.exp(math.log(1.0) - 2.9957323 * jax.random.uniform(key_of[9], (TB, TOP), jnp.float32) ** shard_levels(key_of[9], (TB, TOP), ((0, 8),), -0.2, 0.2)), 0.05, 1.0)
    expert_gain = jnp.clip(1.0 + 0.18 * jax.random.normal(key_of[10], (D,), jnp.float32), 0.1, 1.9)
    gate_weight = centred(key_of[11], (EXPERTS, D, EXPERT_DIM), D ** -0.5, 0.125, ((0, 8), (2, 4)))
    up_weight = centred(key_of[12], (EXPERTS, D, EXPERT_DIM), D ** -0.5, 0.125, ((0, 8), (2, 4)))
    down_weight = centred(key_of[13], (EXPERTS, EXPERT_DIM, D), EXPERT_DIM ** -0.5, 0.09375, ((0, 8), (1, 4)))
    shared_gate = centred(key_of[14], (D, SHARED_DIM), D ** -0.5, 0.125, ((1, 4),))
    shared_up = centred(key_of[15], (D, SHARED_DIM), D ** -0.5, 0.125, ((1, 4),))
    shared_down = centred(key_of[16], (SHARED_DIM, D), SHARED_DIM ** -0.5, 0.125, ((0, 4),))
    return {"query_rows": query_rows, "key_rows": key_rows, "value_rows": value_rows, "query_gain": query_gain, "key_gain": key_gain, "out_weight": out_weight, "mixer_gain": mixer_gain, "expert_input": expert_input, "expert_ids": expert_ids, "gate_score": gate_score, "expert_gain": expert_gain, "gate_weight": gate_weight, "up_weight": up_weight, "down_weight": down_weight, "shared_gate": shared_gate, "shared_up": shared_up, "shared_down": shared_down}


EPSILON = 1e-06
ROUTED_SCALE = 2.5

def rotary_angles(position):
    grid_row = (position // GRID_W).astype(jnp.float32)
    grid_col = (position % GRID_W).astype(jnp.float32)
    quarter = HEAD_DIM // 4
    inverse = 10000.0 ** (-jnp.arange(quarter, dtype=jnp.float32) / quarter)
    return jnp.concatenate([grid_row[:, None] * inverse, grid_col[:, None] * inverse], axis=1)

def normalize_rotate(heads_in, gain_vector, angles):
    widened = heads_in.astype(jnp.float32)
    scaled = widened * lax.rsqrt(lax.optimization_barrier(jnp.mean(widened * widened, axis=-1, keepdims=True)) + EPSILON)
    scaled = scaled * gain_vector.astype(jnp.float32)
    half_dim = scaled.shape[-1] // 2
    front_half = scaled[..., :half_dim]
    back_half = scaled[..., half_dim:]
    cosine_table = jnp.cos(angles)[:, None, :]
    sine_table = jnp.sin(angles)[:, None, :]
    turned = jnp.concatenate([front_half * cosine_table - back_half * sine_table, front_half * sine_table + back_half * cosine_table], axis=-1)
    return turned.astype(jnp.bfloat16)

def swiglu(rows_in, gate_matrix, up_matrix):
    gate_value = jnp.dot(rows_in, gate_matrix, preferred_element_type=jnp.float32)
    up_value = jnp.dot(rows_in, up_matrix, preferred_element_type=jnp.float32)
    return (jax.nn.silu(gate_value) * up_value).astype(jnp.bfloat16)

def lane_sum(hidden, down_matrix):
    group_units = hidden.shape[1] // N_TP

    def add_group(carry, group_index):
        part_hidden = lax.dynamic_slice_in_dim(hidden, group_index * group_units, group_units, 1)
        part_down = lax.dynamic_slice_in_dim(down_matrix, group_index * group_units, group_units, 0)
        partial_value = jnp.dot(part_hidden, part_down, preferred_element_type=jnp.float32).astype(jnp.bfloat16)
        return (carry + lax.optimization_barrier(partial_value).astype(jnp.float32), None)
    start_total = jnp.zeros((hidden.shape[0], down_matrix.shape[1]), jnp.float32)
    total, unused = lax.scan(add_group, start_total, jnp.arange(N_TP, dtype=jnp.int32))
    return total

def fill_slots(empty_table, slot_rows, row_numbers):
    return empty_table.at[slot_rows].set(row_numbers)

def reference(query_rows, key_rows, value_rows, query_gain, key_gain, out_weight, mixer_gain, expert_input, expert_ids, gate_score, expert_gain, gate_weight, up_weight, down_weight, shared_gate, shared_up, shared_down):
    group = HEADS // KV_HEADS
    angles = rotary_angles(jnp.arange(TA, dtype=jnp.int32))
    query_rot = normalize_rotate(query_rows.reshape(TA, HEADS, HEAD_DIM), query_gain, angles)
    key_rot = normalize_rotate(key_rows.reshape(TA, KV_HEADS, HEAD_DIM), key_gain, angles)
    value_heads = value_rows.reshape(TA, KV_HEADS, HEAD_DIM)
    scale_factor = HEAD_DIM ** (-0.5)
    block_count = TA // RA

    def one_head(head_index):
        kv_index = head_index // group
        head_keys = lax.dynamic_index_in_dim(key_rot, kv_index, 1, keepdims=False)
        head_values = lax.dynamic_index_in_dim(value_heads, kv_index, 1, keepdims=False)
        head_queries = lax.dynamic_index_in_dim(query_rot, head_index, 1, keepdims=False)

        def one_block(query_block):
            scores = jnp.dot(query_block, head_keys.T, preferred_element_type=jnp.float32) * scale_factor
            row_peak = lax.optimization_barrier(jnp.max(scores, axis=1, keepdims=True))
            exponent = jnp.exp(scores - row_peak)
            row_total = lax.optimization_barrier(jnp.sum(exponent, axis=1, keepdims=True))
            weighted = jnp.dot(exponent.astype(jnp.bfloat16), head_values, preferred_element_type=jnp.float32)
            return (weighted / row_total).astype(jnp.bfloat16)
        return lax.map(one_block, head_queries.reshape(block_count, RA, HEAD_DIM)).reshape(TA, HEAD_DIM)
    attended = lax.map(one_head, jnp.arange(HEADS, dtype=jnp.int32))
    lane_heads = HEADS // N_TP
    attended_lanes = attended.reshape(N_TP, lane_heads, TA, HEAD_DIM)
    weight_lanes = out_weight.reshape(N_TP, lane_heads, HEAD_DIM, D)

    def add_lane(carry, packed):
        lane_attended, lane_weight = packed
        partial_value = jnp.einsum('hqd,hde->qe', lane_attended.astype(jnp.float32), lane_weight.astype(jnp.float32))
        rounded = lax.optimization_barrier(partial_value.astype(jnp.bfloat16))
        return (carry + rounded.astype(jnp.float32), None)
    mixer_sum, unused = lax.scan(add_lane, jnp.zeros((TA, D), jnp.float32), (attended_lanes, weight_lanes))
    mixer_scale = lax.rsqrt(lax.optimization_barrier(jnp.mean(mixer_sum * mixer_sum, axis=1, keepdims=True)) + EPSILON)
    mixer_out = (mixer_sum * mixer_scale * mixer_gain.astype(jnp.float32)).astype(jnp.bfloat16)
    widened = expert_input.astype(jnp.float32)
    normed = (widened * lax.rsqrt(lax.optimization_barrier(jnp.mean(widened * widened, axis=1, keepdims=True)) + EPSILON) * expert_gain.astype(jnp.float32)).astype(jnp.bfloat16)
    route_weight = gate_score / lax.optimization_barrier(jnp.sum(gate_score, axis=1, keepdims=True)) * ROUTED_SCALE
    pair_ids = expert_ids.reshape(N_EP, RB * TOP)
    onehot = (pair_ids[:, :, None] == jnp.arange(EXPERTS, dtype=jnp.int32)).astype(jnp.int32)
    ranks = lax.optimization_barrier(jnp.sum((jnp.cumsum(onehot, axis=1, dtype=jnp.int32) - 1) * onehot, axis=2, dtype=jnp.int32))
    slot_index = (pair_ids * CAP + ranks).astype(jnp.int32)
    row_numbers = (jnp.arange(N_EP, dtype=jnp.int32)[:, None] * RB + jnp.arange(RB * TOP, dtype=jnp.int32)[None, :] // TOP).astype(jnp.int32)
    sources = jnp.full((N_EP, EXPERTS * CAP), -1, jnp.int32)
    sources = jax.vmap(fill_slots)(sources, slot_index, row_numbers)
    expert_sources = sources.reshape(N_EP, EXPERTS, CAP).transpose(1, 0, 2).reshape(EXPERTS, N_EP * CAP)

    def one_expert(packed):
        source_rows, gate_matrix, up_matrix, down_matrix = packed
        filled = (source_rows >= 0)[:, None]
        picked = jnp.where(filled, normed[jnp.maximum(source_rows, 0)], jnp.zeros((), jnp.bfloat16))
        hidden = swiglu(picked, gate_matrix, up_matrix)
        return lane_sum(hidden, down_matrix).astype(jnp.bfloat16)
    expert_result = lax.map(one_expert, (expert_sources, gate_weight, up_weight, down_weight))
    flat_result = expert_result.reshape(EXPERTS * N_EP * CAP, D)
    block_of = (jnp.arange(TB, dtype=jnp.int32) // RB)[:, None]
    result_index = (expert_ids * (N_EP * CAP) + block_of * CAP + ranks.reshape(TB, TOP)).astype(jnp.int32)
    picked_results = flat_result[result_index]
    routed = lax.optimization_barrier(jnp.sum(picked_results.astype(jnp.float32) * route_weight[:, :, None], axis=1))
    shared_hidden = swiglu(normed, shared_gate, shared_up)
    shared_sum = lane_sum(shared_hidden, shared_down)
    expert_out = (routed + shared_sum).astype(jnp.bfloat16)
    return (mixer_out, expert_out)
```

```python
import functools
import math

import jax
import jax.numpy as jnp
from jax import lax
from jax.experimental import pallas as pl
from jax.experimental.pallas import tpu as pltpu
from jax.sharding import PartitionSpec as P

HEADS = 16
KV_HEADS = 4
HEAD_DIM = 64
GRID_W = 64
EPSILON = 1e-06
ROUTED_SCALE = 2.5
LOG2E = 1.4426950408889634
BF = jnp.bfloat16
F32 = jnp.float32
VMEM = pl.BlockSpec(memory_space=pltpu.VMEM)
SMEM = pl.BlockSpec(memory_space=pltpu.SMEM)


def params(mib):
    return pltpu.CompilerParams(vmem_limit_bytes=mib * 1024 * 1024)


def cost(flops, bytes_accessed, exps=0):
    return pl.CostEstimate(
        flops=int(flops), bytes_accessed=int(bytes_accessed), transcendentals=int(exps)
    )


def dot(a, b, dims=((1,), (0,))):
    return lax.dot_general(a, b, (dims, ((), ())), preferred_element_type=F32)


def rotary_table(offset, local_rows):
    grid_rows = local_rows // GRID_W
    quarter = HEAD_DIM // 4
    inverse = 10000.0 ** (-jnp.arange(quarter, dtype=F32) / quarter)
    inverse = jnp.tile(inverse, 128 // quarter)[None, :]
    rows = (offset // GRID_W + jnp.arange(grid_rows, dtype=jnp.int32)).astype(F32)
    cols = jnp.arange(GRID_W, dtype=jnp.int32).astype(F32)
    angle = jnp.concatenate([rows, cols])[:, None] * inverse
    sign = jnp.where(jnp.arange(128) % HEAD_DIM < HEAD_DIM // 2, -1.0, 1.0).astype(F32)[None, :]
    return jnp.concatenate([jnp.cos(angle), jnp.sin(angle) * sign], axis=0)


def rotate_block(x, gain, table_ref, grid_rows, g):
    lane = lax.broadcasted_iota(jnp.int32, x.shape, 1)
    squares = x * x
    first = lane < HEAD_DIM
    sum_a = jnp.sum(jnp.where(first, squares, 0.0), axis=1, keepdims=True)
    sum_b = jnp.sum(jnp.where(first, 0.0, squares), axis=1, keepdims=True)
    mean = jnp.where(first, sum_a, sum_b) * (1.0 / HEAD_DIM)
    y = x * lax.rsqrt(mean + EPSILON) * gain
    by_row = lane % 32 < 16
    height = grid_rows + GRID_W
    cosine = jnp.where(by_row, table_ref[g : g + 1, :], table_ref[grid_rows:height, :])
    sine = jnp.where(
        by_row,
        table_ref[height + g : height + g + 1, :],
        table_ref[height + grid_rows : 2 * height, :],
    )
    swapped = jnp.where(lane % HEAD_DIM < 32, pltpu.roll(y, 96, 1), pltpu.roll(y, 32, 1))
    return y * cosine + swapped * sine


def key_kernel(grid_rows, parity_ref, key_ref, value_ref, gain_ref, table_ref, out_ref):
    odd = parity_ref[1] == 1
    lane = lax.broadcasted_iota(jnp.int32, (GRID_W, 128), 1)
    for g in range(grid_rows):
        rows = slice(g * GRID_W, (g + 1) * GRID_W)
        keys = key_ref[rows, :].astype(F32)
        values = value_ref[rows, :].astype(F32)
        turned = rotate_block(keys, gain_ref[...], table_ref, grid_rows, g)
        turned = jnp.where(odd, pltpu.roll(turned, 64, 1), turned)
        values = jnp.where(odd, values, pltpu.roll(values, 64, 1))
        out_ref[rows, :] = jnp.where(lane < HEAD_DIM, turned, values).astype(BF)


def prepare_keys(key_rows, value_rows, gain, table, kv_index):
    local_rows = key_rows.shape[0]
    grid_rows = local_rows // GRID_W
    place = jnp.stack([kv_index // 2, kv_index % 2]).astype(jnp.int32)
    return pl.pallas_call(
        functools.partial(key_kernel, grid_rows),
        grid_spec=pltpu.PrefetchScalarGridSpec(
            num_scalar_prefetch=1,
            grid=(1,),
            in_specs=[
                pl.BlockSpec((local_rows, 128), lambda i, s: (0, s[0])),
                pl.BlockSpec((local_rows, 128), lambda i, s: (0, s[0])),
                pl.BlockSpec((1, 128), lambda i, s: (0, 0)),
                pl.BlockSpec(table.shape, lambda i, s: (0, 0)),
            ],
            out_specs=pl.BlockSpec((local_rows, 128), lambda i, s: (0, 0)),
        ),
        out_shape=jax.ShapeDtypeStruct((local_rows, 128), BF),
        cost_estimate=cost(1e6, 3e5),
        name="keys",
    )(place, key_rows, value_rows, gain, table)


def attention_kernel(
    heads, halves, tile, chunk, side_ref, q_ref, *rest
):
    n_kv = len(rest) - 9
    kv_refs = rest[:n_kv]
    gain_ref, table_ref, w_ref, send_ref, keep_ref, qs_ref, s_ref, o_ref, att_ref = rest[n_kv:]
    local_rows = q_ref.shape[0]
    grid_rows = local_rows // GRID_W
    lane = lax.broadcasted_iota(jnp.int32, (GRID_W, 128), 1)
    for pair in range(q_ref.shape[1] // 128):
        for g in range(grid_rows):
            x = q_ref[g * GRID_W : (g + 1) * GRID_W, pair * 128 : (pair + 1) * 128].astype(F32)
            turned = rotate_block(x, gain_ref[...], table_ref, grid_rows, g)
            turned = turned.astype(BF).astype(F32) * HEAD_DIM ** (-0.5)
            for k in range(2):
                head = pair * 2 + k
                if head < heads:
                    own = turned if k == 0 else pltpu.roll(turned, 64, 1)
                    start = head * local_rows + g * GRID_W
                    qs_ref[start : start + GRID_W, :] = jnp.where(lane < HEAD_DIM, own, 0.0).astype(BF)
    pieces = []
    column = 0
    for ref in kv_refs:
        for b in range(ref.shape[0]):
            for start in range(0, ref.shape[1], chunk):
                pieces.append((ref, b, start, column))
                column += chunk

    def one_tile(i, unused):
        begin = pl.multiple_of(i * tile, tile)
        q = qs_ref[pl.ds(begin, tile), :]
        peak = None
        for ref, b, start, at in pieces:
            s = dot(q, ref[b, start : start + chunk, :], ((1,), (1,)))
            s_ref[:, at : at + chunk] = s
            for c in range(0, chunk, 128):
                part = s[:, c : c + 128]
                peak = part if peak is None else jnp.maximum(peak, part)
        peak = jnp.max(peak, axis=1, keepdims=True)
        total = jnp.zeros((tile, 128), F32)
        accum = jnp.zeros((tile, 128), F32)
        for ref, b, start, at in pieces:
            e = jnp.exp2((s_ref[:, at : at + chunk] - peak) * LOG2E)
            for c in range(0, chunk, 128):
                total = total + e[:, c : c + 128]
            accum = accum + dot(e.astype(BF), ref[b, start : start + chunk, :])
        o_ref[pl.ds(begin, tile), :] = accum / jnp.sum(total, axis=1, keepdims=True)
        return unused

    lax.fori_loop(0, heads * local_rows // tile, one_tile, 0)
    wide = lax.broadcasted_iota(jnp.int32, (local_rows, 128), 1)
    for pair in range(q_ref.shape[1] // 128):
        head = pair * 2
        low = pltpu.roll(o_ref[head * local_rows : (head + 1) * local_rows, :], 64, 1)
        high = (
            o_ref[(head + 1) * local_rows : (head + 2) * local_rows, :]
            if head + 1 < heads
            else jnp.zeros((local_rows, 128), F32)
        )
        att_ref[:, pair * 128 : (pair + 1) * 128] = jnp.where(wide < HEAD_DIM, low, high).astype(BF)
    share = local_rows // (2 * halves)
    side = side_ref[0]
    for y in range(halves):
        for core, out in ((1 - side, send_ref), (side, keep_ref)):
            begin = pl.multiple_of((2 * y + core) * share, 8)
            out[y] = dot(att_ref[pl.ds(begin, share), :], w_ref[...]).astype(BF)


def attention(query_rows, kv_list, gain, table, out_weight, side, halves):
    local_rows, width = query_rows.shape
    heads = width // HEAD_DIM
    if width % 128:
        query_rows = jnp.pad(query_rows, ((0, 0), (0, 64)))
        out_weight = jnp.pad(out_weight, ((0, 64), (0, 0)))
    keys = sum(k.shape[0] * k.shape[1] for k in kv_list)
    tile = 128
    chunk = 384
    share = local_rows // (2 * halves)
    model = out_weight.shape[1]
    shape = jax.ShapeDtypeStruct((halves, share, model), BF)
    return pl.pallas_call(
        functools.partial(attention_kernel, heads, halves, tile, chunk),
        in_specs=[SMEM] + [VMEM] * (len(kv_list) + 4),
        out_specs=[VMEM, VMEM],
        out_shape=[shape, shape],
        scratch_shapes=[
            pltpu.VMEM((heads * local_rows, 128), BF),
            pltpu.VMEM((tile, keys), F32),
            pltpu.VMEM((heads * local_rows, 128), F32),
            pltpu.VMEM((local_rows, query_rows.shape[1]), BF),
        ],
        compiler_params=params(48),
        cost_estimate=cost(8e9, 4e6, heads * local_rows * keys),
        name="attention",
    )(side, query_rows, *kv_list, gain, table, out_weight)


def route_kernel(experts, cap, lane_ref, ids_ref, idst_ref, x_ref, gain_ref, *outs):
    normed_ref, slot_ref = outs[:2]
    chunk_refs = outs[2:]
    rows, top = ids_ref.shape
    x = x_ref[...].astype(F32)
    mean = jnp.mean(x * x, axis=1, keepdims=True)
    normed_ref[...] = (x * lax.rsqrt(mean + EPSILON) * gain_ref[...]).astype(BF)
    names = lax.broadcasted_iota(jnp.int32, (rows, experts), 1)
    hits = [ids_ref[:, k : k + 1] == names for k in range(top)]
    named = functools.reduce(jnp.logical_or, hits)
    r0 = lax.broadcasted_iota(jnp.int32, (rows, rows), 0)
    r1 = lax.broadcasted_iota(jnp.int32, (rows, rows), 1)
    below = jnp.where(r1 < r0, 1.0, 0.0).astype(BF)
    above = jnp.where(r0 < r1, 1.0, 0.0).astype(BF)
    count = dot(below, jnp.where(named, 1.0, 0.0).astype(BF))
    columns = []
    for k in range(top):
        rank = jnp.sum(jnp.where(hits[k], count, 0.0), axis=1, keepdims=True)
        columns.append(ids_ref[:, k : k + 1] * cap + rank.astype(jnp.int32))
    for k in range(top):
        slot_ref[:, k : k + 1] = columns[k]
    namest = lax.broadcasted_iota(jnp.int32, (experts, rows), 0)
    namedt = functools.reduce(
        jnp.logical_or, [idst_ref[k : k + 1, :] == namest for k in range(top)]
    )
    countt = dot(jnp.where(namedt, 1.0, 0.0).astype(BF), above).astype(jnp.int32)
    place = jnp.where(namedt, countt, -1)
    width = chunk_refs[0].shape[2]
    own = normed_ref[:, pl.ds(pl.multiple_of(lane_ref[0] * width, 128), width)]
    size = cap // len(chunk_refs)
    slots = lax.broadcasted_iota(jnp.int32, (cap, rows), 0)
    for e in range(experts):
        pick = jnp.where(place[e : e + 1, :] == slots, 1.0, 0.0).astype(BF)
        moved = dot(pick, own).astype(BF)
        for h, ref in enumerate(chunk_refs):
            ref[e] = moved[h * size : (h + 1) * size, :]


def route(expert_ids, expert_input, gain, lane, experts, cap, chunks, width):
    rows, top = expert_ids.shape
    model = expert_input.shape[1]
    return pl.pallas_call(
        functools.partial(route_kernel, experts, cap),
        in_specs=[SMEM] + [VMEM] * 4,
        out_specs=[VMEM] * (2 + chunks),
        out_shape=[
            jax.ShapeDtypeStruct((rows, model), BF),
            jax.ShapeDtypeStruct((rows, top), jnp.int32),
        ]
        + [jax.ShapeDtypeStruct((experts, cap // chunks, width), BF)] * chunks,
        compiler_params=params(32),
        cost_estimate=cost(1e9, 4e6),
        name="route",
    )(lane, expert_ids, expert_ids.T, expert_input, gain)


def mlp_kernel(n_x, halves, place_ref, *refs):
    x_refs = refs[:n_x]
    gate_ref, up_ref, down_ref, send_ref, keep_ref, x_scr, acc_ref = refs[n_x:]
    step = pl.program_id(0)
    rows = x_scr.shape[0]

    @pl.when(step == 0)
    def assemble():
        at = 0
        for ref in x_refs:
            for b in range(ref.shape[0]):
                width = ref.shape[2]
                begin = pl.multiple_of(place_ref[1 + at] * width, 128)
                x_scr[:, pl.ds(begin, width)] = ref[b]
                at += 1

    x = x_scr[...]
    gate = dot(x, gate_ref[0])
    up = dot(x, up_ref[0])
    hidden = (gate / (1.0 + jnp.exp(-gate)) * up).astype(BF)
    part = dot(hidden, down_ref[0])

    @pl.when(step == 0)
    def first():
        acc_ref[...] = part

    @pl.when(step > 0)
    def later():
        acc_ref[...] += part

    @pl.when(step == pl.num_programs(0) - 1)
    def finish():
        side = place_ref[0]
        width = send_ref.shape[2]
        for y in range(halves):
            for core, out in ((1 - side, send_ref), (side, keep_ref)):
                begin = pl.multiple_of((2 * y + core) * width, 128)
                out[y] = acc_ref[:, pl.ds(begin, width)].astype(BF)


def mlp(x_list, gate, up, down, place, halves):
    rows = x_list[0].shape[1]
    model, hidden = gate.shape[1:]
    block = min(256, hidden)
    width = model // (2 * halves)
    shape = jax.ShapeDtypeStruct((halves, rows, width), BF)

    def full(a):
        return pl.BlockSpec(a.shape, lambda i, s: (0, 0, 0))

    return pl.pallas_call(
        functools.partial(mlp_kernel, len(x_list), halves),
        grid_spec=pltpu.PrefetchScalarGridSpec(
            num_scalar_prefetch=1,
            grid=(hidden // block,),
            in_specs=[full(a) for a in x_list]
            + [
                pl.BlockSpec((1, model, block), lambda i, s: (0, 0, i)),
                pl.BlockSpec((1, model, block), lambda i, s: (0, 0, i)),
                pl.BlockSpec((1, block, model), lambda i, s: (0, i, 0)),
            ],
            out_specs=[pl.BlockSpec(shape.shape, lambda i, s: (0, 0, 0))] * 2,
            scratch_shapes=[pltpu.VMEM((rows, model), BF), pltpu.VMEM((rows, model), F32)],
        ),
        out_shape=[shape, shape],
        compiler_params=params(48),
        cost_estimate=cost(6 * rows * model * hidden, 6 * model * hidden),
        name="mlp",
    )(place, *x_list, gate, up, down)


def combine_kernel(cap, chunks, slot_ref, score_ref, *refs):
    chunk_refs = refs[:chunks]
    shared_a, shared_b, out_ref = refs[chunks:]
    rows, top = slot_ref.shape
    experts, size, width = chunk_refs[0].shape
    scores = score_ref[...]
    weight = scores / jnp.sum(scores, axis=1, keepdims=True) * ROUTED_SCALE
    n = lax.broadcasted_iota(jnp.int32, (rows, experts * size), 1)
    routed = None
    for k in range(top):
        slot = slot_ref[:, k : k + 1]
        expert = slot // cap
        inside = slot - expert * cap
        picked = None
        for h, ref in enumerate(chunk_refs):
            fits = (inside >= h * size) & (inside < (h + 1) * size)
            at = jnp.where(fits, expert * size + inside - h * size, -1)
            pick = jnp.where(n == at, 1.0, 0.0).astype(BF)
            got = dot(pick, ref[...].reshape(experts * size, width))
            picked = got if picked is None else picked + got
        term = picked * weight[:, k : k + 1]
        routed = term if routed is None else routed + term
    shared = shared_a[...] + shared_b[...].astype(F32)
    out_ref[...] = (routed + shared).astype(BF)


def combine(slot, gate_score, chunk_list, shared_a, shared_b, cap):
    rows = slot.shape[0]
    width = chunk_list[0].shape[2]
    return pl.pallas_call(
        functools.partial(combine_kernel, cap, len(chunk_list)),
        in_specs=[VMEM] * (4 + len(chunk_list)),
        out_specs=VMEM,
        out_shape=jax.ShapeDtypeStruct((rows, width), BF),
        compiler_params=params(32),
        cost_estimate=cost(8e8, 2e6),
        name="combine",
    )(slot, gate_score, *chunk_list, shared_a, shared_b)


def core_swap(x):
    n = lax.axis_size("tp")
    return lax.ppermute(x, "tp", [(i, i ^ 1) for i in range(n)])


def chip_shift(x, step):
    n = lax.axis_size("tp")
    return lax.ppermute(x, "tp", [(i, (i + 2 * step) % n) for i in range(n)])


def scatter_chips(keep, received, chip, halves):
    total = lax.dynamic_index_in_dim(keep, chip, 0, False).astype(F32)
    total = total + lax.dynamic_index_in_dim(received, chip, 0, False).astype(F32)
    arrived = []
    for step in range(1, halves):
        to = (chip + step) % halves
        term = lax.dynamic_index_in_dim(keep, to, 0, False).astype(F32)
        term = term + lax.dynamic_index_in_dim(received, to, 0, False).astype(F32)
        arrived.append(chip_shift(term.astype(BF), step))
    for a in arrived[:-1]:
        total = total + a.astype(F32)
    return total, arrived[-1]


def gather_chips(x, halves):
    return [x[None]] + [chip_shift(x, step)[None] for step in range(1, halves)]


def ep_gather(x, axis_z, axis_x):
    n = lax.axis_size("ep")
    own = [x]
    for step in range(1, axis_z):
        own.append(lax.ppermute(x, "ep", [(i, (i + step * axis_x) % n) for i in range(n)]))
    stacked = jnp.stack(own)
    groups = [stacked]
    for step in range(1, axis_x):
        perm = [(i, i // axis_x * axis_x + (i + step) % axis_x) for i in range(n)]
        groups.append(lax.ppermute(stacked, "ep", perm))
    return groups


def body(
    x_size,
    query_rows,
    key_rows,
    value_rows,
    query_gain,
    key_gain,
    out_weight,
    mixer_gain,
    expert_input,
    expert_ids,
    gate_score,
    expert_gain,
    gate_weight,
    up_weight,
    down_weight,
    shared_gate,
    shared_up,
    shared_down,
):
    ep, tp = lax.axis_size("ep"), lax.axis_size("tp")
    halves = tp // 2
    lane = lax.axis_index("tp")
    chip, side = lane // 2, lane % 2
    local_rows = query_rows.shape[0]
    heads = query_rows.shape[1] // HEAD_DIM
    assert tp % 2 == 0 and heads <= HEADS // KV_HEADS and gate_weight.shape[0] == 1
    rows, top = expert_ids.shape
    model = expert_input.shape[1]
    width = model // tp
    cap = 3 * rows * top // (2 * ep)
    chunks = 2

    table = rotary_table(lax.axis_index("ep") * local_rows, local_rows)
    key_gain2 = jnp.tile(key_gain, 2)[None, :]
    query_gain2 = jnp.tile(query_gain, 2)[None, :]
    kv_index = lane * heads * KV_HEADS // HEADS
    kv = prepare_keys(key_rows, value_rows, key_gain2, table, kv_index)
    kv_list = ep_gather(kv, ep // x_size, x_size)

    lane_s = lane[None].astype(jnp.int32)
    side_s = side[None].astype(jnp.int32)
    normed, slot, *outgoing = route(
        expert_ids, expert_input, expert_gain[None, :], lane_s, ep, cap, chunks, width
    )
    arrived = [lax.all_to_all(o, "ep", 0, 0, tiled=True) for o in outgoing]

    identity = jnp.concatenate([side_s, jnp.zeros((1,), jnp.int32)])
    sh_send, sh_keep = mlp(
        [normed[None]], shared_gate[None], shared_up[None], shared_down[None], identity, halves
    )
    sh_total, sh_last = scatter_chips(sh_keep, core_swap(sh_send), chip, halves)

    send, keep = attention(
        query_rows, kv_list, query_gain2, table, out_weight, side_s, halves
    )

    chips = [(chip - step) % halves for step in range(halves)]
    place = jnp.stack(
        [side] + [2 * c + side for c in chips] + [2 * c + 1 - side for c in chips]
    ).astype(jnp.int32)
    returned = []
    for a in arrived:
        x = a.reshape(ep * (cap // chunks), width)
        mine = gather_chips(x, halves)
        mine = jnp.concatenate(mine, axis=0)
        other = core_swap(mine)
        d_send, d_keep = mlp([mine, other], gate_weight, up_weight, down_weight, place, halves)
        total, last = scatter_chips(d_keep, core_swap(d_send), chip, halves)
        result = (total + last.astype(F32)).astype(BF).reshape(ep, cap // chunks, width)
        returned.append(lax.all_to_all(result, "ep", 0, 0, tiled=True))

    total, last = scatter_chips(keep, core_swap(send), chip, halves)
    mixer_sum = total + last.astype(F32)
    scale = lax.rsqrt(jnp.mean(mixer_sum * mixer_sum, axis=1, keepdims=True) + EPSILON)
    mixed = (mixer_sum * scale * mixer_gain).astype(BF)
    mine = jnp.concatenate(gather_chips(mixed, halves), axis=0)
    other = core_swap(mine)
    pieces = jnp.where(side == 0, jnp.stack([mine, other], 1), jnp.stack([other, mine], 1))
    back = (chip - jnp.arange(halves)) % halves
    mixer_out = pieces[back].reshape(local_rows, model)

    expert_out = combine(slot, gate_score, returned, sh_total, sh_last, cap)
    return (mixer_out, expert_out)


def solution(mesh):
    in_specs = (
        P("ep", "tp"),
        P("ep", None),
        P("ep", None),
        P(),
        P(),
        P("tp", None),
        P(),
        P("ep", None),
        P("ep", None),
        P("ep", None),
        P(),
        P("ep", None, "tp"),
        P("ep", None, "tp"),
        P("ep", "tp", None),
        P(None, "tp"),
        P(None, "tp"),
        P("tp", None),
    )
    out_specs = (P("ep", None), P("ep", "tp"))
    ep = mesh.shape["ep"]
    x_size = 2 ** (int(math.log2(ep)) // 2)
    return jax.shard_map(
        functools.partial(body, x_size),
        mesh=mesh,
        in_specs=in_specs,
        out_specs=out_specs,
        check_vma=False,
    )
```

```python
import functools
import math

import jax
import jax.numpy as jnp
import numpy as np
from jax import lax
from jax.experimental import pallas as pl
from jax.experimental.pallas import tpu as pltpu
from jax.sharding import PartitionSpec as P


HEADS = 16
KV_HEADS = 4
HEAD_DIM = 64
GRID_W = 64
EPSILON = 1e-06
ROUTED_SCALE = 2.5
LOG2E = 1.4426950408889634
BF = jnp.bfloat16
F32 = jnp.float32
VMEM = pl.BlockSpec(memory_space=pltpu.VMEM)
HBM = pl.BlockSpec(memory_space=pltpu.HBM)


def params(mib):
    return pltpu.CompilerParams(vmem_limit_bytes=mib * 1024 * 1024)


def cost(flops, bytes_accessed, exps=0):
    return pl.CostEstimate(
        flops=int(flops), bytes_accessed=int(bytes_accessed), transcendentals=int(exps)
    )


def in_hbm(arrays):
    return [pltpu.with_memory_space_constraint(a, pltpu.HBM) for a in arrays]


def fetch(sources, targets, sems):
    copies = [
        pltpu.make_async_copy(a, b, sems.at[i]) for i, (a, b) in enumerate(zip(sources, targets))
    ]
    for copy in copies:
        copy.start()
    return copies


def wait(copies):
    for copy in copies:
        copy.wait()


def room(arrays):
    return [pltpu.VMEM(a.shape, a.dtype) for a in arrays] + [
        pltpu.SemaphoreType.DMA((len(arrays),))
    ]


def dot(a, b, dims=((1,), (0,))):
    return lax.dot_general(a, b, (dims, ((), ())), preferred_element_type=F32)


def rotate_block(x, gain, table_ref, grid_rows, g):
    lane = lax.broadcasted_iota(jnp.int32, x.shape, 1)
    squares = x * x
    first = lane < HEAD_DIM
    sum_a = jnp.sum(jnp.where(first, squares, 0.0), axis=1, keepdims=True)
    sum_b = jnp.sum(jnp.where(first, 0.0, squares), axis=1, keepdims=True)
    mean = jnp.where(first, sum_a, sum_b) * (1.0 / HEAD_DIM)
    y = x * lax.rsqrt(mean + EPSILON) * gain
    by_row = lane % 32 < 16
    height = grid_rows + GRID_W
    cosine = jnp.where(by_row, table_ref[g : g + 1, :], table_ref[grid_rows:height, :])
    sine = jnp.where(
        by_row,
        table_ref[height + g : height + g + 1, :],
        table_ref[height + grid_rows : 2 * height, :],
    )
    swapped = jnp.where(lane % HEAD_DIM < 32, pltpu.roll(y, 96, 1), pltpu.roll(y, 32, 1))
    return y * cosine + swapped * sine


def key_kernel(
    heads, key_hbm, value_hbm, gain_hbm, inverse_hbm, out_ref, table_ref, key_ref, value_ref,
    gain_ref, inverse_ref, sems,
):
    kv_index = lax.axis_index("tp") * heads * KV_HEADS // HEADS
    cols = pl.ds(pl.multiple_of(kv_index // 2 * 128, 128), 128)
    copies = fetch(
        [inverse_hbm, gain_hbm, key_hbm.at[:, cols], value_hbm.at[:, cols]],
        [inverse_ref, gain_ref, key_ref, value_ref],
        sems,
    )
    wait(copies[:1])
    local_rows = key_ref.shape[0]
    grid_rows = local_rows // GRID_W
    height = grid_rows + GRID_W
    index = lax.broadcasted_iota(jnp.int32, (height, 128), 0)
    place = jnp.where(
        index < grid_rows, lax.axis_index("ep") * grid_rows + index, index - grid_rows
    )
    angle = place.astype(F32) * inverse_ref[...]
    lanes = lax.broadcasted_iota(jnp.int32, (height, 128), 1)
    table_ref[:height, :] = jnp.cos(angle)
    sine = jnp.sin(angle)
    table_ref[height:, :] = jnp.where(lanes % HEAD_DIM < HEAD_DIM // 2, -sine, sine)
    odd = kv_index % 2 == 1
    wait(copies[1:])
    gain = jnp.concatenate([gain_ref[...]] * 2, axis=1)
    lane = lax.broadcasted_iota(jnp.int32, (GRID_W, 128), 1)
    for g in range(grid_rows):
        rows = slice(g * GRID_W, (g + 1) * GRID_W)
        keys = key_ref[rows, :].astype(F32)
        values = value_ref[rows, :].astype(F32)
        turned = rotate_block(keys, gain, table_ref, grid_rows, g)
        turned = jnp.where(odd, pltpu.roll(turned, 64, 1), turned)
        values = jnp.where(odd, values, pltpu.roll(values, 64, 1))
        out_ref[rows, :] = jnp.where(lane < HEAD_DIM, turned, values).astype(BF)


def prepare_keys(key_rows, value_rows, gain, heads):
    local_rows = key_rows.shape[0]
    height = local_rows // GRID_W + GRID_W
    quarter = HEAD_DIM // 4
    inverse = 10000.0 ** (-np.arange(quarter, dtype=np.float32) / quarter)
    inverse = jnp.asarray(np.tile(inverse, 128 // quarter)[None, :], F32)
    args = (key_rows, value_rows, gain[None, :], inverse)
    return pl.pallas_call(
        functools.partial(key_kernel, heads),
        in_specs=[HBM] * 4,
        out_specs=[VMEM] * 2,
        out_shape=[
            jax.ShapeDtypeStruct((local_rows, 128), BF),
            jax.ShapeDtypeStruct((2 * height, 128), F32),
        ],
        scratch_shapes=[pltpu.VMEM((local_rows, 128), BF)] * 2 + room(args[2:])[:2]
        + [pltpu.SemaphoreType.DMA((4,))],
        compiler_params=params(8),
        cost_estimate=cost(1e9, 3e5),
        name="keys",
    )(*in_hbm(args))


def attention_kernel(heads, tile, chunk, n_kv, q_hbm, gain_hbm, table_hbm, *rest):
    kv_refs = rest[:n_kv]
    att_ref, qs_ref, sa_ref, sb_ref, o_ref, kt_ref, q_ref, gain_ref, table_ref, sems = rest[n_kv:]
    copies = fetch([q_hbm, gain_hbm, table_hbm], [q_ref, gain_ref, table_ref], sems)
    local_rows = q_ref.shape[0]
    grid_rows = local_rows // GRID_W
    blocks = [ref.at[b] for ref in kv_refs for b in range(ref.shape[0])]
    for i, ref in enumerate(blocks):
        kt_ref[:, i * local_rows : (i + 1) * local_rows] = ref[...].astype(F32).T.astype(BF)
    keys = len(blocks) * local_rows
    wait(copies)
    lane = lax.broadcasted_iota(jnp.int32, (GRID_W, 128), 1)
    gain = jnp.concatenate([gain_ref[...]] * 2, axis=1)
    pairs = q_ref.shape[1] // 128
    for pair in range(pairs):
        for g in range(grid_rows):
            x = q_ref[g * GRID_W : (g + 1) * GRID_W, pair * 128 : (pair + 1) * 128].astype(F32)
            turned = rotate_block(x, gain, table_ref, grid_rows, g)
            turned = turned.astype(BF).astype(F32) * HEAD_DIM ** (-0.5)
            for k in range(min(2, heads - 2 * pair)):
                own = turned if k == 0 else pltpu.roll(turned, 64, 1)
                start = (2 * pair + k) * local_rows + g * GRID_W
                qs_ref[start : start + GRID_W, :] = jnp.where(lane < HEAD_DIM, own, 0.0).astype(BF)

    def score(q, s_ref, at, peak):
        s = dot(q, kt_ref[:, at : at + chunk]) * LOG2E
        s_ref[:, at : at + chunk] = s
        for c in range(0, chunk, 128):
            part = s[:, c : c + 128]
            peak = part if peak is None else jnp.maximum(peak, part)
        return peak

    tiles = heads * local_rows // tile
    buffers = (sa_ref, sb_ref)
    peak = None
    for at in range(0, keys, chunk):
        peak = score(qs_ref[:tile, :], sa_ref, at, peak)
    peak = jnp.max(peak, axis=1, keepdims=True)
    for i in range(tiles):
        begin = i * tile
        total = jnp.zeros((tile, 128), F32)
        accum = jnp.zeros((tile, 128), F32)
        next_peak = None
        for at in range(0, keys, chunk):
            if i + 1 < tiles:
                q = qs_ref[begin + tile : begin + 2 * tile, :]
                next_peak = score(q, buffers[(i + 1) % 2], at, next_peak)
            e = jnp.exp2(buffers[i % 2][:, at : at + chunk] - peak)
            for c in range(0, chunk, 128):
                total = total + e[:, c : c + 128]
            e = e.astype(BF)
            for c in range(0, chunk, local_rows):
                accum = accum + dot(e[:, c : c + local_rows], blocks[(at + c) // local_rows][...])
        o_ref[begin : begin + tile, :] = accum / jnp.sum(total, axis=1, keepdims=True)
        if i + 1 < tiles:
            peak = jnp.max(next_peak, axis=1, keepdims=True)
    wide = lax.broadcasted_iota(jnp.int32, (local_rows, 128), 1)
    for pair in range(pairs):
        start = 2 * pair * local_rows
        low = pltpu.roll(o_ref[start : start + local_rows, :], 64, 1)
        if heads > 2 * pair + 1:
            high = o_ref[start + local_rows : start + 2 * local_rows, :]
        else:
            high = jnp.zeros((local_rows, 128), F32)
        att_ref[:, pair * 128 : (pair + 1) * 128] = jnp.where(wide < HEAD_DIM, low, high).astype(BF)


def attention(query_rows, kv_list, gain, table):
    local_rows, width = query_rows.shape
    heads = width // HEAD_DIM
    if width % 128:
        query_rows = jnp.pad(query_rows, ((0, 0), (0, 64)))
    keys = sum(k.shape[0] * k.shape[1] for k in kv_list)
    chunk = 2 * local_rows if keys % (2 * local_rows) == 0 else local_rows
    tile = 256 if heads * local_rows % 256 == 0 else 128
    args = (query_rows, gain[None, :], table)
    attended = pl.pallas_call(
        functools.partial(attention_kernel, heads, tile, chunk, len(kv_list)),
        in_specs=[HBM] * 3 + [VMEM] * len(kv_list),
        out_specs=VMEM,
        out_shape=jax.ShapeDtypeStruct(query_rows.shape, BF),
        scratch_shapes=[
            pltpu.VMEM((heads * local_rows, 128), BF),
            pltpu.VMEM((tile, keys), F32),
            pltpu.VMEM((tile, keys), F32),
            pltpu.VMEM((heads * local_rows, 128), F32),
            pltpu.VMEM((128, keys), BF),
        ]
        + room(args),
        compiler_params=params(24),
        cost_estimate=cost(8e9, 2e6, heads * local_rows * keys),
        name="attention",
    )(*in_hbm(args), *kv_list)
    return attended[:, :width]


def project_kernel(counts, block, *refs):
    att_refs, rest = refs[: len(counts)], refs[len(counts) :]
    w_refs = []
    for count in counts:
        w_refs.append(rest[:count])
        rest = rest[count:]
    gain_ref, out_ref, sum_ref = rest
    rows, model = out_ref.shape
    squares = jnp.zeros((rows, 128), F32)
    for at in range(0, model, block):
        total = None
        for a, parts in zip(att_refs, w_refs):
            part, row = None, 0
            for w in parts:
                term = dot(a[:, row : row + w.shape[0]], w[:, at : at + block])
                part = term if part is None else part + term
                row += w.shape[0]
            part = part.astype(BF).astype(F32)
            total = part if total is None else total + part
        sum_ref[:, at : at + block] = total
        for c in range(0, block, 128):
            squares = squares + total[:, c : c + 128] * total[:, c : c + 128]
    mean = jnp.sum(squares, axis=1, keepdims=True) * (1.0 / model)
    scale = lax.rsqrt(mean + EPSILON)
    for at in range(0, model, block):
        cols = slice(at, at + block)
        out_ref[:, cols] = (sum_ref[:, cols] * scale * gain_ref[:, cols]).astype(BF)


def project(att_list, w_list, gain):
    rows, model = att_list[0].shape[0], w_list[0][0].shape[1]
    args = (*att_list, *(w for parts in w_list for w in parts), gain[None, :])
    return pl.pallas_call(
        functools.partial(project_kernel, [len(w) for w in w_list], min(256, model)),
        in_specs=[VMEM] * len(args),
        out_specs=VMEM,
        out_shape=jax.ShapeDtypeStruct((rows, model), BF),
        scratch_shapes=[pltpu.VMEM((rows, model), F32)],
        compiler_params=params(32),
        cost_estimate=cost(2e9, 6e6),
        name="project",
    )(*args)


def route_kernel(
    experts, cap, ids_hbm, score_hbm, x_hbm, gain_hbm, normed_ref, plan_hbm, out_hbm, plan_ref,
    out_ref, idst_ref, score_ref, x_ref, gain_ref, sems, out_sems,
):
    copies = fetch(
        [ids_hbm, score_hbm, gain_hbm, x_hbm], [idst_ref, score_ref, gain_ref, x_ref], sems
    )
    wait(copies[:2])
    top, rows = idst_ref.shape
    names = lax.broadcasted_iota(jnp.int32, (experts, rows), 0)
    hits = [idst_ref[k : k + 1, :] == names for k in range(top)]
    named = functools.reduce(jnp.logical_or, hits)
    r0 = lax.broadcasted_iota(jnp.int32, (rows, rows), 0)
    r1 = lax.broadcasted_iota(jnp.int32, (rows, rows), 1)
    above = jnp.where(r0 < r1, 1.0, 0.0).astype(BF)
    count = dot(jnp.where(named, 1.0, 0.0).astype(BF), above)
    scores = [score_ref[k : k + 1, :] for k in range(top)]
    score_sum = functools.reduce(jnp.add, scores)
    lines = []
    for k in range(top):
        rank = jnp.sum(jnp.where(hits[k], count, 0.0), axis=0, keepdims=True)
        lines.append((idst_ref[k : k + 1, :] * cap).astype(F32) + rank)
    lines += [s / score_sum * ROUTED_SCALE for s in scores]
    lines += [jnp.zeros((8 - 2 * top, rows), F32)]
    plan_ref[...] = jnp.concatenate(lines, axis=0).T
    sent = [pltpu.make_async_copy(plan_ref, plan_hbm, out_sems.at[0])]
    sent[0].start()
    wait(copies[2:])
    x = x_ref[...].astype(F32)
    mean = jnp.mean(x * x, axis=1, keepdims=True)
    normed_ref[...] = (x * lax.rsqrt(mean + EPSILON) * gain_ref[...]).astype(BF)
    place = jnp.where(named, count.astype(jnp.int32), -1)
    width = out_ref.shape[2]
    lane = lax.axis_index("tp")
    own = normed_ref[:, pl.ds(pl.multiple_of(lane * width, 128), width)]
    slots = lax.broadcasted_iota(jnp.int32, (cap, rows), 0)
    for e in range(experts):
        pick = jnp.where(place[e : e + 1, :] == slots, 1.0, 0.0).astype(BF)
        out_ref[e] = dot(pick, own).astype(BF)
        sent.append(pltpu.make_async_copy(out_ref.at[e], out_hbm.at[e], out_sems.at[1 + e]))
        sent[-1].start()
    wait(sent)


def route(expert_ids, gate_score, expert_input, gain, experts, cap, width):
    rows = expert_ids.shape[0]
    args = (expert_ids.T, gate_score.T, expert_input, gain[None, :])
    outs = [
        jax.ShapeDtypeStruct(expert_input.shape, BF),
        jax.ShapeDtypeStruct((rows, 8), F32),
        jax.ShapeDtypeStruct((experts, cap, width), BF),
    ]
    return pl.pallas_call(
        functools.partial(route_kernel, experts, cap),
        in_specs=[HBM] * 4,
        out_specs=[VMEM, HBM, HBM],
        out_shape=outs[:1] + [pltpu.HBM(a.shape, a.dtype) for a in outs[1:]],
        scratch_shapes=room(outs[1:])[:2]
        + room(args)
        + [pltpu.SemaphoreType.DMA((experts + 1,))],
        compiler_params=params(16),
        cost_estimate=cost(1e9, 4e6),
        name="route",
    )(*in_hbm(args))


def loads_of(hidden):
    return 2 if hidden % 512 == 0 else 1


def mlp_kernel(n_x, halves, offsets, early, late, chunk, *refs):
    x_refs, refs = refs[:n_x], refs[n_x:]
    if late:
        partial_ref, refs = refs[0], refs[1:]
    gate_hbm, up_hbm, refs = refs[0], refs[1], refs[2:]
    if early:
        out_ref, gate_ref, up_ref, sems = refs
    else:
        down_hbm, send_ref, keep_ref, gate_ref, up_ref, sems, h_ref, down_ref = refs
    lane = lax.axis_index("tp")
    chip, side = lane // 2, lane % 2
    hidden = gate_ref.shape[1]
    block = min(256, hidden // loads_of(hidden))
    rows, row = [], 0
    for ref, offset in zip(x_refs, offsets):
        size = ref.shape[1]
        begin = 0
        if offset is not None:
            source = 2 * lax.rem(chip + halves - offset[0], halves)
            source = source + (side if offset[1] == 0 else 1 - side)
            begin = pl.multiple_of(source * size, 128)
        rows.append((pl.ds(begin, size), slice(row, row + size)))
        row += size
    loads = loads_of(hidden)
    load = hidden // loads
    groups = []
    for at in range(0, hidden, load):
        cols = slice(at, at + load)
        groups.append(
            [
                (w_hbm.at[0, there, cols], w_ref.at[here, cols])
                for w_hbm, w_ref in ((gate_hbm, gate_ref), (up_hbm, up_ref))
                for there, here in rows
            ]
        )
    if not early:
        width = send_ref.shape[2]
        goals = [(1 - side, step, send_ref) for step in range(halves)]
        goals += [(side, step, keep_ref) for step in range(halves)]
        groups.append([])
        for i, (core, step, unused) in enumerate(goals):
            goal = 2 * lax.rem(chip + step, halves) + core
            begin = pl.multiple_of(goal * width, 128)
            groups[-1].append((down_hbm.at[0, :, pl.ds(begin, width)], down_ref.at[i]))
    number = 0
    for i, group in enumerate(groups):
        groups[i] = [
            pltpu.make_async_copy(x, y, sems.at[number + j]) for j, (x, y) in enumerate(group)
        ]
        number += len(group)

    def start(i):
        for copy in groups[i] if i < len(groups) else ():
            copy.start()

    start(0)
    if loads > 1:
        start(1)

    def product(w_ref, cols):
        total = None
        for ref, (unused, here) in zip(x_refs, rows):
            term = dot(ref[...], w_ref[here, cols])
            total = term if total is None else total + term
        return total

    for at in range(0, hidden, block):
        cols = slice(at, at + block)
        if at % load == 0:
            wait(groups[at // load])
            start(at // load + min(2, loads))
        gate = product(gate_ref, cols)
        up = product(up_ref, cols)
        if late:
            taken = slice(chunk * gate.shape[0], (chunk + 1) * gate.shape[0])
            gate = gate + partial_ref[0, taken, cols]
            up = up + partial_ref[1, taken, cols]
        if early:
            out_ref[0, :, cols] = gate
            out_ref[1, :, cols] = up
        else:
            h_ref[:, cols] = (gate / (1.0 + jnp.exp(-gate)) * up).astype(BF)
    if early:
        return
    inner = min(256, width)
    wait(groups[-1])
    for i, (unused, step, out) in enumerate(goals):
        for at in range(0, width, inner):
            cols = slice(at, at + inner)
            out[step, :, cols] = dot(h_ref[...], down_ref[i, :, cols]).astype(BF)


def mlp(x_list, offsets, weights, halves, early=False, partial=None, chunk=0):
    rows = x_list[0].shape[0]
    model, hidden = weights[0].shape[1:]
    width = model // (2 * halves)
    depth = sum(x.shape[1] for x in x_list)
    n_copies = 2 * len(x_list) * loads_of(hidden)
    if early:
        weights = weights[:2]
        outs = [jax.ShapeDtypeStruct((2, rows, hidden), F32)]
    else:
        n_copies += 2 * halves
        outs = [jax.ShapeDtypeStruct((halves, rows, width), BF)] * 2
    scratch = [pltpu.VMEM((depth, hidden), BF)] * 2 + [pltpu.SemaphoreType.DMA((n_copies,))]
    if not early:
        scratch += [pltpu.VMEM((rows, hidden), BF), pltpu.VMEM((2 * halves, hidden, width), BF)]
    late = [] if partial is None else [partial]
    flops = 4 * rows * depth * hidden + (0 if early else 2 * rows * model * hidden)
    return pl.pallas_call(
        functools.partial(mlp_kernel, len(x_list), halves, offsets, early, bool(late), chunk),
        in_specs=[VMEM] * len(x_list + late) + [HBM] * len(weights),
        out_specs=[VMEM] * len(outs),
        out_shape=outs,
        scratch_shapes=scratch,
        compiler_params=params(24),
        cost_estimate=cost(flops, 6 * model * hidden),
    )(*x_list, *late, *in_hbm(weights))


def small_call(kernel, args, outs, scratch=()):
    return pl.pallas_call(
        kernel,
        in_specs=[VMEM] * len(args),
        out_specs=[HBM if isinstance(o, type(pltpu.HBM((8, 128), F32))) else VMEM for o in outs],
        out_shape=outs,
        scratch_shapes=list(scratch),
        compiler_params=params(4),
        cost_estimate=cost(1e8, 2e6),
    )(*args)


def split_kernel(in_ref, *outs):
    for i, out in enumerate(outs):
        out[...] = in_ref[i]


def split(x):
    shape = jax.ShapeDtypeStruct(x.shape[1:], x.dtype)
    return small_call(split_kernel, [x], [shape] * x.shape[0])


def stack_kernel(*refs):
    for i, ref in enumerate(refs[:-1]):
        refs[-1][i] = ref[...]


def stack(arrays):
    shape = jax.ShapeDtypeStruct((len(arrays), *arrays[0].shape), arrays[0].dtype)
    return small_call(stack_kernel, arrays, [shape])[0]


def add_kernel(a_ref, b_ref, *outs):
    for i, out in enumerate(outs):
        out[...] = (a_ref[1 + i].astype(F32) + b_ref[1 + i].astype(F32)).astype(BF)


def add_terms(keep, received):
    shape = jax.ShapeDtypeStruct(keep.shape[1:], BF)
    return small_call(add_kernel, [keep, received], [shape] * (keep.shape[0] - 1))


def finish_kernel(counts, *refs):
    refs, out_hbm, out_ref, sems = refs[:-3], refs[-3], refs[-2], refs[-1]
    width = out_ref.shape[2]
    blocks = out_ref.shape[0] // len(counts)
    copies = []
    for h, count in enumerate(counts):
        keep, received, others = refs[0], refs[1], refs[2:count]
        refs = refs[count:]
        total = keep[0].astype(F32) + received[0].astype(F32)
        for other in others:
            total = total + other[...].astype(F32)
        at = h * blocks
        out_ref[at : at + blocks] = total.astype(BF).reshape(blocks, out_ref.shape[1], width)
        copies.append(
            pltpu.make_async_copy(
                out_ref.at[at : at + blocks], out_hbm.at[at : at + blocks], sems.at[h]
            )
        )
        copies[-1].start()
    wait(copies)


def finish(groups, shape):
    return small_call(
        functools.partial(finish_kernel, [len(g) for g in groups]),
        [a for g in groups for a in g],
        [pltpu.HBM(shape, BF)],
        [pltpu.VMEM(shape, BF), pltpu.SemaphoreType.DMA((shape[0],))],
    )[0]


def combine_kernel(top, plan_hbm, slots_ref, keep_ref, received_ref, *refs):
    others, (out_ref, plan_ref, sems) = refs[:-3], refs[-3:]
    copies = fetch([plan_hbm], [plan_ref], sems)
    rows = plan_ref.shape[0]
    experts, cap, width = slots_ref.shape
    n = lax.broadcasted_iota(jnp.int32, (rows, experts * cap), 1)
    total = keep_ref[0].astype(F32) + received_ref[0].astype(F32)
    for other in others:
        total = total + other[...].astype(F32)
    wait(copies)
    for k in range(top):
        pick = jnp.where(n == plan_ref[:, k : k + 1].astype(jnp.int32), 1.0, 0.0).astype(BF)
        picked = dot(pick, slots_ref[...].reshape(experts * cap, width))
        total = total + picked * plan_ref[:, top + k : top + k + 1]
    out_ref[...] = total.astype(BF)


def combine(plan, top, slots, keep, received, others):
    rows = plan.shape[0]
    args = (slots, keep, received, *others)
    return pl.pallas_call(
        functools.partial(combine_kernel, top),
        in_specs=[HBM] + [VMEM] * len(args),
        out_specs=VMEM,
        out_shape=jax.ShapeDtypeStruct((rows, slots.shape[2]), BF),
        scratch_shapes=room([plan]),
        compiler_params=params(16),
        cost_estimate=cost(8e8, 2e6),
        name="combine",
    )(*in_hbm([plan]), *args)


def core_swap(x):
    n = lax.axis_size("tp")
    return lax.ppermute(x, "tp", [(i, i ^ 1) for i in range(n)])


def chip_shift(x, step):
    n = lax.axis_size("tp")
    return lax.ppermute(x, "tp", [(i, (i + 2 * step) % n) for i in range(n)])


def gather_lanes(x, halves):
    mine = [x] + [chip_shift(x, s) for s in range(1, halves)]
    other = [core_swap(m) for m in mine]
    offsets = [(s, 0) for s in range(halves)] + [(s, 1) for s in range(halves)]
    return mine + other, offsets


def scatter_chips(keep, received):
    terms = add_terms(keep, received)
    return [chip_shift(t, s + 1) for s, t in enumerate(terms)]


def ep_gather(x, axis_z, axis_x):
    n = lax.axis_size("ep")
    own = [x]
    for step in range(1, axis_z):
        own.append(lax.ppermute(x, "ep", [(i, (i + step * axis_x) % n) for i in range(n)]))
    stacked = stack(own)
    groups = [stacked]
    for step in range(1, axis_x):
        perm = [(i, i // axis_x * axis_x + (i + step) % axis_x) for i in range(n)]
        groups.append(lax.ppermute(stacked, "ep", perm))
    return groups


def exchange(x):
    return lax.all_to_all(x, "ep", 0, 0, tiled=True)


def body(
    x_size,
    query_rows,
    key_rows,
    value_rows,
    query_gain,
    key_gain,
    out_weight,
    mixer_gain,
    expert_input,
    expert_ids,
    gate_score,
    expert_gain,
    gate_weight,
    up_weight,
    down_weight,
    shared_gate,
    shared_up,
    shared_down,
):
    return whole_step(
        x_size,
        query_rows,
        key_rows,
        value_rows,
        query_gain,
        key_gain,
        out_weight,
        mixer_gain,
        expert_input,
        expert_ids,
        gate_score,
        expert_gain,
        gate_weight,
        up_weight,
        down_weight,
        shared_gate,
        shared_up,
        shared_down,
    )


def whole_step(
    x_size,
    query_rows,
    key_rows,
    value_rows,
    query_gain,
    key_gain,
    out_weight,
    mixer_gain,
    expert_input,
    expert_ids,
    gate_score,
    expert_gain,
    gate_weight,
    up_weight,
    down_weight,
    shared_gate,
    shared_up,
    shared_down,
):
    ep, tp = lax.axis_size("ep"), lax.axis_size("tp")
    halves = tp // 2
    heads = query_rows.shape[1] // HEAD_DIM
    assert tp > 2 and tp % 2 == 0 and heads <= HEADS // KV_HEADS and gate_weight.shape[0] == 1
    rows, top = expert_ids.shape
    width = expert_input.shape[1] // tp
    cap = 3 * rows * top // (2 * ep)
    chunks = 2
    size = ep * cap // chunks

    part = out_weight.shape[0] // 8 * 7
    parts = [out_weight[:part], out_weight[part:]]
    w_list = [[out_weight]]
    for step in range(1, halves):
        w_list.append([chip_shift(w, step) for w in parts])
    w_list += [[core_swap(w) for w in parts] for parts in w_list]

    normed, plan, outgoing = route(
        expert_ids, gate_score, expert_input, expert_gain, ep, cap, width
    )
    arrived = exchange(outgoing).reshape(chunks * size, width)

    shared = (shared_gate[None], shared_up[None], shared_down[None])
    sh_send, sh_keep = mlp([normed], [None], shared, halves)
    sh_received = core_swap(sh_send)
    sh_others = scatter_chips(sh_keep, sh_received)

    weights = [gate_weight, up_weight, down_weight]
    own_chip = [arrived, core_swap(arrived)]
    (partial,) = mlp(own_chip, [(0, 0), (0, 1)], weights, halves, True)
    results = []
    for h, x in enumerate(split(arrived.reshape(chunks, size, width))):
        mine = [chip_shift(x, s) for s in range(1, halves)]
        other = [core_swap(m) for m in mine]
        offsets = [(s, c) for c in range(2) for s in range(1, halves)]
        send, keep = mlp(mine + other, offsets, weights, halves, partial=partial, chunk=h)
        received = core_swap(send)
        results.append((keep, received, *scatter_chips(keep, received)))
    returned = exchange(finish(results, (ep, cap, width)))
    expert_out = combine(plan, top, returned, sh_keep, sh_received, sh_others)

    kv, table = prepare_keys(key_rows, value_rows, key_gain, heads)
    kv_list = ep_gather(kv, ep // x_size, x_size)
    attended = attention(query_rows, kv_list, query_gain, table)[:, : query_rows.shape[1]]
    att_list, _ = gather_lanes(attended, halves)
    mixer_out = project(att_list, w_list, mixer_gain)
    return (mixer_out, expert_out)


def solution(mesh):
    in_specs = (
        P("ep", "tp"),
        P("ep", None),
        P("ep", None),
        P(),
        P(),
        P("tp", None),
        P(),
        P("ep", None),
        P("ep", None),
        P("ep", None),
        P(),
        P("ep", None, "tp"),
        P("ep", None, "tp"),
        P("ep", "tp", None),
        P(None, "tp"),
        P(None, "tp"),
        P("tp", None),
    )
    out_specs = (P("ep", None), P("ep", "tp"))
    ep = mesh.shape["ep"]
    x_size = 2 ** (int(math.log2(ep)) // 2)
    return jax.shard_map(
        functools.partial(body, x_size),
        mesh=mesh,
        in_specs=in_specs,
        out_specs=out_specs,
        check_vma=False,
    )
```

```python
import functools
import math

import jax
import jax.numpy as jnp
import numpy as np
from jax import lax
from jax.experimental import pallas as pl
from jax.experimental.pallas import tpu as pltpu
from jax.sharding import PartitionSpec as P


HEADS = 16
KV_HEADS = 4
HEAD_DIM = 64
GRID_W = 64
EPSILON = 1e-06
ROUTED_SCALE = 2.5
LOG2E = 1.4426950408889634
BF = jnp.bfloat16
F32 = jnp.float32
VMEM = pl.BlockSpec(memory_space=pltpu.VMEM)
HBM = pl.BlockSpec(memory_space=pltpu.HBM)


def params(mib):
    return pltpu.CompilerParams(vmem_limit_bytes=mib * 1024 * 1024)


def cost(flops, bytes_accessed, exps=0):
    return pl.CostEstimate(
        flops=int(flops), bytes_accessed=int(bytes_accessed), transcendentals=int(exps)
    )


def in_hbm(arrays):
    return [pltpu.with_memory_space_constraint(a, pltpu.HBM) for a in arrays]


def fetch(sources, targets, sems):
    copies = [
        pltpu.make_async_copy(a, b, sems.at[i]) for i, (a, b) in enumerate(zip(sources, targets))
    ]
    for copy in copies:
        copy.start()
    return copies


def wait(copies):
    for copy in copies:
        copy.wait()


def room(arrays):
    return [pltpu.VMEM(a.shape, a.dtype) for a in arrays] + [
        pltpu.SemaphoreType.DMA((len(arrays),))
    ]


def dot(a, b, dims=((1,), (0,))):
    return lax.dot_general(a, b, (dims, ((), ())), preferred_element_type=F32)


def rotate_block(x, gain, table_ref, grid_rows, g):
    lane = lax.broadcasted_iota(jnp.int32, x.shape, 1)
    squares = x * x
    first = lane < HEAD_DIM
    sum_a = jnp.sum(jnp.where(first, squares, 0.0), axis=1, keepdims=True)
    sum_b = jnp.sum(jnp.where(first, 0.0, squares), axis=1, keepdims=True)
    mean = jnp.where(first, sum_a, sum_b) * (1.0 / HEAD_DIM)
    y = x * lax.rsqrt(mean + EPSILON) * gain
    by_row = lane % 32 < 16
    height = grid_rows + GRID_W
    cosine = jnp.where(by_row, table_ref[g : g + 1, :], table_ref[grid_rows:height, :])
    sine = jnp.where(
        by_row,
        table_ref[height + g : height + g + 1, :],
        table_ref[height + grid_rows : 2 * height, :],
    )
    swapped = jnp.where(lane % HEAD_DIM < 32, pltpu.roll(y, 96, 1), pltpu.roll(y, 32, 1))
    return y * cosine + swapped * sine


def key_kernel(
    heads, key_hbm, value_hbm, gain_hbm, inverse_hbm, out_ref, table_ref, key_ref, value_ref,
    gain_ref, inverse_ref, sems,
):
    kv_index = lax.axis_index("tp") * heads * KV_HEADS // HEADS
    cols = pl.ds(pl.multiple_of(kv_index // 2 * 128, 128), 128)
    copies = fetch(
        [inverse_hbm, gain_hbm, key_hbm.at[:, cols], value_hbm.at[:, cols]],
        [inverse_ref, gain_ref, key_ref, value_ref],
        sems,
    )
    wait(copies[:1])
    local_rows = key_ref.shape[0]
    grid_rows = local_rows // GRID_W
    height = grid_rows + GRID_W
    index = lax.broadcasted_iota(jnp.int32, (height, 128), 0)
    place = jnp.where(
        index < grid_rows, lax.axis_index("ep") * grid_rows + index, index - grid_rows
    )
    angle = place.astype(F32) * inverse_ref[...]
    lanes = lax.broadcasted_iota(jnp.int32, (height, 128), 1)
    table_ref[:height, :] = jnp.cos(angle)
    sine = jnp.sin(angle)
    table_ref[height:, :] = jnp.where(lanes % HEAD_DIM < HEAD_DIM // 2, -sine, sine)
    odd = kv_index % 2 == 1
    wait(copies[1:])
    gain = jnp.concatenate([gain_ref[...]] * 2, axis=1)
    lane = lax.broadcasted_iota(jnp.int32, (GRID_W, 128), 1)
    for g in range(grid_rows):
        rows = slice(g * GRID_W, (g + 1) * GRID_W)
        keys = key_ref[rows, :].astype(F32)
        values = value_ref[rows, :].astype(F32)
        turned = rotate_block(keys, gain, table_ref, grid_rows, g)
        turned = jnp.where(odd, pltpu.roll(turned, 64, 1), turned)
        values = jnp.where(odd, values, pltpu.roll(values, 64, 1))
        out_ref[rows, :] = jnp.where(lane < HEAD_DIM, turned, values).astype(BF)


def prepare_keys(key_rows, value_rows, gain, heads):
    local_rows = key_rows.shape[0]
    height = local_rows // GRID_W + GRID_W
    quarter = HEAD_DIM // 4
    inverse = 10000.0 ** (-np.arange(quarter, dtype=np.float32) / quarter)
    inverse = jnp.asarray(np.tile(inverse, 128 // quarter)[None, :], F32)
    args = (key_rows, value_rows, gain[None, :], inverse)
    return pl.pallas_call(
        functools.partial(key_kernel, heads),
        in_specs=[HBM] * 4,
        out_specs=[VMEM] * 2,
        out_shape=[
            jax.ShapeDtypeStruct((local_rows, 128), BF),
            jax.ShapeDtypeStruct((2 * height, 128), F32),
        ],
        scratch_shapes=[pltpu.VMEM((local_rows, 128), BF)] * 2 + room(args[2:])[:2]
        + [pltpu.SemaphoreType.DMA((4,))],
        compiler_params=params(8),
        cost_estimate=cost(1e9, 3e5),
        name="keys",
    )(*in_hbm(args))


def attention_kernel(heads, tile, chunk, n_kv, q_hbm, gain_hbm, table_hbm, *rest):
    kv_refs = rest[:n_kv]
    att_ref, qs_ref, sa_ref, sb_ref, o_ref, kt_ref, q_ref, gain_ref, table_ref, sems = rest[n_kv:]
    copies = fetch([q_hbm, gain_hbm, table_hbm], [q_ref, gain_ref, table_ref], sems)
    local_rows = q_ref.shape[0]
    grid_rows = local_rows // GRID_W
    blocks = [ref.at[b] for ref in kv_refs for b in range(ref.shape[0])]
    for i, ref in enumerate(blocks):
        kt_ref[:, i * local_rows : (i + 1) * local_rows] = ref[...].astype(F32).T.astype(BF)
    keys = len(blocks) * local_rows
    wait(copies)
    lane = lax.broadcasted_iota(jnp.int32, (GRID_W, 128), 1)
    gain = jnp.concatenate([gain_ref[...]] * 2, axis=1)
    pairs = q_ref.shape[1] // 128
    for pair in range(pairs):
        for g in range(grid_rows):
            x = q_ref[g * GRID_W : (g + 1) * GRID_W, pair * 128 : (pair + 1) * 128].astype(F32)
            turned = rotate_block(x, gain, table_ref, grid_rows, g)
            turned = turned.astype(BF).astype(F32) * HEAD_DIM ** (-0.5)
            for k in range(min(2, heads - 2 * pair)):
                own = turned if k == 0 else pltpu.roll(turned, 64, 1)
                start = (2 * pair + k) * local_rows + g * GRID_W
                qs_ref[start : start + GRID_W, :] = jnp.where(lane < HEAD_DIM, own, 0.0).astype(BF)

    def score(q, s_ref, at, peak):
        s = dot(q, kt_ref[:, at : at + chunk]) * LOG2E
        s_ref[:, at : at + chunk] = s
        for c in range(0, chunk, 128):
            part = s[:, c : c + 128]
            peak = part if peak is None else jnp.maximum(peak, part)
        return peak

    tiles = heads * local_rows // tile
    buffers = (sa_ref, sb_ref)
    peak = None
    for at in range(0, keys, chunk):
        peak = score(qs_ref[:tile, :], sa_ref, at, peak)
    peak = jnp.max(peak, axis=1, keepdims=True)
    for i in range(tiles):
        begin = i * tile
        total = jnp.zeros((tile, 128), F32)
        accum = jnp.zeros((tile, 128), F32)
        next_peak = None
        for at in range(0, keys, chunk):
            if i + 1 < tiles:
                q = qs_ref[begin + tile : begin + 2 * tile, :]
                next_peak = score(q, buffers[(i + 1) % 2], at, next_peak)
            e = jnp.exp2(buffers[i % 2][:, at : at + chunk] - peak)
            for c in range(0, chunk, 128):
                total = total + e[:, c : c + 128]
            e = e.astype(BF)
            for c in range(0, chunk, local_rows):
                accum = accum + dot(e[:, c : c + local_rows], blocks[(at + c) // local_rows][...])
        o_ref[begin : begin + tile, :] = accum / jnp.sum(total, axis=1, keepdims=True)
        if i + 1 < tiles:
            peak = jnp.max(next_peak, axis=1, keepdims=True)
    wide = lax.broadcasted_iota(jnp.int32, (local_rows, 128), 1)
    for pair in range(pairs):
        start = 2 * pair * local_rows
        low = pltpu.roll(o_ref[start : start + local_rows, :], 64, 1)
        if heads > 2 * pair + 1:
            high = o_ref[start + local_rows : start + 2 * local_rows, :]
        else:
            high = jnp.zeros((local_rows, 128), F32)
        att_ref[:, pair * 128 : (pair + 1) * 128] = jnp.where(wide < HEAD_DIM, low, high).astype(BF)


def attention(query_rows, kv_list, gain, table):
    local_rows, width = query_rows.shape
    heads = width // HEAD_DIM
    if width % 128:
        query_rows = jnp.pad(query_rows, ((0, 0), (0, 64)))
    keys = sum(k.shape[0] * k.shape[1] for k in kv_list)
    chunk = 2 * local_rows if keys % (2 * local_rows) == 0 else local_rows
    tile = 256 if heads * local_rows % 256 == 0 else 128
    args = (query_rows, gain[None, :], table)
    attended = pl.pallas_call(
        functools.partial(attention_kernel, heads, tile, chunk, len(kv_list)),
        in_specs=[HBM] * 3 + [VMEM] * len(kv_list),
        out_specs=VMEM,
        out_shape=jax.ShapeDtypeStruct(query_rows.shape, BF),
        scratch_shapes=[
            pltpu.VMEM((heads * local_rows, 128), BF),
            pltpu.VMEM((tile, keys), F32),
            pltpu.VMEM((tile, keys), F32),
            pltpu.VMEM((heads * local_rows, 128), F32),
            pltpu.VMEM((128, keys), BF),
        ]
        + room(args),
        compiler_params=params(24),
        cost_estimate=cost(8e9, 2e6, heads * local_rows * keys),
        name="attention",
    )(*in_hbm(args), *kv_list)
    return attended[:, :width]


def project_kernel(counts, block, *refs):
    att_refs, rest = refs[: len(counts)], refs[len(counts) :]
    w_refs = []
    for count in counts:
        w_refs.append(rest[:count])
        rest = rest[count:]
    gain_ref, out_ref, sum_ref = rest
    rows, model = out_ref.shape
    squares = jnp.zeros((rows, 128), F32)
    for at in range(0, model, block):
        total = None
        for a, parts in zip(att_refs, w_refs):
            part, row = None, 0
            for w in parts:
                term = dot(a[:, row : row + w.shape[0]], w[:, at : at + block])
                part = term if part is None else part + term
                row += w.shape[0]
            part = part.astype(BF).astype(F32)
            total = part if total is None else total + part
        sum_ref[:, at : at + block] = total
        for c in range(0, block, 128):
            squares = squares + total[:, c : c + 128] * total[:, c : c + 128]
    mean = jnp.sum(squares, axis=1, keepdims=True) * (1.0 / model)
    scale = lax.rsqrt(mean + EPSILON)
    for at in range(0, model, block):
        cols = slice(at, at + block)
        out_ref[:, cols] = (sum_ref[:, cols] * scale * gain_ref[:, cols]).astype(BF)


def project(att_list, w_list, gain):
    rows, model = att_list[0].shape[0], w_list[0][0].shape[1]
    args = (*att_list, *(w for parts in w_list for w in parts), gain[None, :])
    return pl.pallas_call(
        functools.partial(project_kernel, [len(w) for w in w_list], min(256, model)),
        in_specs=[VMEM] * len(args),
        out_specs=VMEM,
        out_shape=jax.ShapeDtypeStruct((rows, model), BF),
        scratch_shapes=[pltpu.VMEM((rows, model), F32)],
        compiler_params=params(32),
        cost_estimate=cost(2e9, 6e6),
        name="project",
    )(*args)


def route_kernel(
    experts, cap, ids_hbm, score_hbm, x_hbm, gain_hbm, normed_ref, plan_hbm, *refs
):
    out_refs = refs[:experts]
    plan_ref, place_ref, idst_ref, score_ref, x_ref, gain_ref, sems, out_sem = refs[experts:]
    copies = fetch(
        [ids_hbm, score_hbm, gain_hbm, x_hbm], [idst_ref, score_ref, gain_ref, x_ref], sems
    )
    wait(copies[:2])
    top, rows = idst_ref.shape
    names = lax.broadcasted_iota(jnp.int32, (experts, rows), 0)
    hits = [idst_ref[k : k + 1, :] == names for k in range(top)]
    named = functools.reduce(jnp.logical_or, hits)
    r0 = lax.broadcasted_iota(jnp.int32, (rows, rows), 0)
    r1 = lax.broadcasted_iota(jnp.int32, (rows, rows), 1)
    above = jnp.where(r0 < r1, 1.0, 0.0).astype(BF)
    count = dot(jnp.where(named, 1.0, 0.0).astype(BF), above)
    scores = [score_ref[k : k + 1, :] for k in range(top)]
    score_sum = functools.reduce(jnp.add, scores)
    lines = []
    for k in range(top):
        rank = jnp.sum(jnp.where(hits[k], count, 0.0), axis=0, keepdims=True)
        lines.append((idst_ref[k : k + 1, :] * cap).astype(F32) + rank)
    lines += [s / score_sum * ROUTED_SCALE for s in scores]
    lines += [jnp.zeros((8 - 2 * top, rows), F32)]
    plan_ref[...] = jnp.concatenate(lines, axis=0).T
    sent = pltpu.make_async_copy(plan_ref, plan_hbm, out_sem)
    sent.start()
    place_ref[...] = jnp.where(named, count.astype(jnp.int32), -1)
    wait(copies[2:])
    x = x_ref[...].astype(F32)
    mean = jnp.mean(x * x, axis=1, keepdims=True)
    normed_ref[...] = (x * lax.rsqrt(mean + EPSILON) * gain_ref[...]).astype(BF)
    width = out_refs[0].shape[1]
    own = normed_ref[:, pl.ds(pl.multiple_of(lax.axis_index("tp") * width, 128), width)]
    slots = lax.broadcasted_iota(jnp.int32, (cap, rows), 0)
    me = lax.axis_index("ep")
    for step, ref in enumerate(out_refs):
        place = place_ref[pl.ds(me ^ step, 1), :]
        ref[...] = dot(jnp.where(place == slots, 1.0, 0.0).astype(BF), own).astype(BF)
    sent.wait()


def route(expert_ids, gate_score, expert_input, gain, experts, cap, width):
    rows = expert_ids.shape[0]
    args = (expert_ids.T, gate_score.T, expert_input, gain[None, :])
    normed = jax.ShapeDtypeStruct(expert_input.shape, BF)
    block = jax.ShapeDtypeStruct((cap, width), BF)
    return pl.pallas_call(
        functools.partial(route_kernel, experts, cap),
        in_specs=[HBM] * 4,
        out_specs=[VMEM, HBM] + [VMEM] * experts,
        out_shape=[normed, pltpu.HBM((rows, 8), F32)] + [block] * experts,
        scratch_shapes=[pltpu.VMEM((rows, 8), F32), pltpu.VMEM((experts, rows), jnp.int32)]
        + room(args)
        + [pltpu.SemaphoreType.DMA],
        compiler_params=params(16),
        cost_estimate=cost(1e9, 4e6),
        name="route",
    )(*in_hbm(args))


def loads_of(hidden):
    return 2 if hidden % 512 == 0 else 1


def mlp_kernel(n_x, halves, offsets, early, late, chunk, *refs):
    x_refs, refs = refs[:n_x], refs[n_x:]
    if late:
        partial_ref, refs = refs[0], refs[1:]
    gate_hbm, up_hbm, refs = refs[0], refs[1], refs[2:]
    if early:
        out_ref, gate_ref, up_ref, sems = refs
    else:
        down_hbm, send_ref, keep_ref, gate_ref, up_ref, sems, h_ref, down_ref = refs
    lane = lax.axis_index("tp")
    chip, side = lane // 2, lane % 2
    hidden = gate_ref.shape[1]
    block = min(256, hidden // loads_of(hidden))
    rows, row = [], 0
    for ref, offset in zip(x_refs, offsets):
        size = ref.shape[1]
        begin = 0
        if offset is not None:
            source = 2 * lax.rem(chip + halves - offset[0], halves)
            source = source + (side if offset[1] == 0 else 1 - side)
            begin = pl.multiple_of(source * size, 128)
        rows.append((pl.ds(begin, size), slice(row, row + size)))
        row += size
    loads = loads_of(hidden)
    load = hidden // loads
    groups = []
    for at in range(0, hidden, load):
        cols = slice(at, at + load)
        groups.append(
            [
                (w_hbm.at[0, there, cols], w_ref.at[here, cols])
                for w_hbm, w_ref in ((gate_hbm, gate_ref), (up_hbm, up_ref))
                for there, here in rows
            ]
        )
    if not early:
        width = send_ref.shape[2]
        goals = [(1 - side, step, send_ref) for step in range(halves)]
        goals += [(side, step, keep_ref) for step in range(halves)]
        groups.append([])
        for i, (core, step, unused) in enumerate(goals):
            goal = 2 * lax.rem(chip + step, halves) + core
            begin = pl.multiple_of(goal * width, 128)
            groups[-1].append((down_hbm.at[0, :, pl.ds(begin, width)], down_ref.at[i]))
    number = 0
    for i, group in enumerate(groups):
        groups[i] = [
            pltpu.make_async_copy(x, y, sems.at[number + j]) for j, (x, y) in enumerate(group)
        ]
        number += len(group)

    def start(i):
        for copy in groups[i] if i < len(groups) else ():
            copy.start()

    start(0)
    if loads > 1:
        start(1)

    def product(w_ref, cols, x_refs):
        total = None
        for ref, (unused, here) in zip(x_refs, rows):
            term = dot(ref[...], w_ref[here, cols])
            total = term if total is None else total + term
        return total

    for at in range(0, hidden, block):
        cols = slice(at, at + block)
        if at % load == 0:
            wait(groups[at // load])
            start(at // load + min(2, loads))
        for h in range(0, n_x, len(offsets)):
            gate = product(gate_ref, cols, x_refs[h : h + len(offsets)])
            up = product(up_ref, cols, x_refs[h : h + len(offsets)])
            if early:
                taken = slice(h // len(offsets) * gate.shape[0], (h // len(offsets) + 1) * gate.shape[0])
                out_ref[0, taken, cols] = gate
                out_ref[1, taken, cols] = up
                continue
            if late:
                taken = slice(chunk * gate.shape[0], (chunk + 1) * gate.shape[0])
                gate = gate + partial_ref[0, taken, cols]
                up = up + partial_ref[1, taken, cols]
            h_ref[:, cols] = (gate / (1.0 + jnp.exp(-gate)) * up).astype(BF)
    if early:
        return
    inner = min(256, width)
    wait(groups[-1])
    for i, (unused, step, out) in enumerate(goals):
        for at in range(0, width, inner):
            cols = slice(at, at + inner)
            out[step, :, cols] = dot(h_ref[...], down_ref[i, :, cols]).astype(BF)


def mlp(x_list, offsets, weights, halves, early=False, partial=None, chunk=0):
    rows = x_list[0].shape[0]
    model, hidden = weights[0].shape[1:]
    width = model // (2 * halves)
    depth = sum(x.shape[1] for x in x_list[: len(offsets)])
    n_copies = 2 * len(offsets) * loads_of(hidden)
    if early:
        weights = weights[:2]
        outs = [jax.ShapeDtypeStruct((2, len(x_list) // len(offsets) * rows, hidden), F32)]
    else:
        n_copies += 2 * halves
        outs = [jax.ShapeDtypeStruct((halves, rows, width), BF)] * 2
    scratch = [pltpu.VMEM((depth, hidden), BF)] * 2 + [pltpu.SemaphoreType.DMA((n_copies,))]
    if not early:
        scratch += [pltpu.VMEM((rows, hidden), BF), pltpu.VMEM((2 * halves, hidden, width), BF)]
    late = [] if partial is None else [partial]
    flops = 4 * rows * depth * hidden + (0 if early else 2 * rows * model * hidden)
    return pl.pallas_call(
        functools.partial(mlp_kernel, len(x_list), halves, offsets, early, bool(late), chunk),
        in_specs=[VMEM] * len(x_list + late) + [HBM] * len(weights),
        out_specs=[VMEM] * len(outs),
        out_shape=outs,
        scratch_shapes=scratch,
        compiler_params=params(24),
        cost_estimate=cost(flops, 6 * model * hidden),
    )(*x_list, *late, *in_hbm(weights))


def small_call(kernel, args, outs, scratch=()):
    return pl.pallas_call(
        kernel,
        in_specs=[VMEM] * len(args),
        out_specs=[HBM if isinstance(o, type(pltpu.HBM((8, 128), F32))) else VMEM for o in outs],
        out_shape=outs,
        scratch_shapes=list(scratch),
        compiler_params=params(4),
        cost_estimate=cost(1e8, 2e6),
    )(*args)


def stack_kernel(*refs):
    for i, ref in enumerate(refs[:-1]):
        refs[-1][i] = ref[...]


def stack(arrays):
    shape = jax.ShapeDtypeStruct((len(arrays), *arrays[0].shape), arrays[0].dtype)
    return small_call(stack_kernel, arrays, [shape])[0]


def add_kernel(a_ref, b_ref, *outs):
    for i, out in enumerate(outs):
        out[...] = (a_ref[1 + i].astype(F32) + b_ref[1 + i].astype(F32)).astype(BF)


def add_terms(keep, received):
    shape = jax.ShapeDtypeStruct(keep.shape[1:], BF)
    return small_call(add_kernel, [keep, received], [shape] * (keep.shape[0] - 1))


def finish_kernel(counts, *refs):
    refs, out_hbm, out_ref, sems = refs[:-3], refs[-3], refs[-2], refs[-1]
    ep, cap, width = out_ref.shape
    blocks = ep // len(counts)
    me = lax.axis_index("ep")
    copies = []
    for h, count in enumerate(counts):
        keep, received, others = refs[0], refs[1], refs[2:count]
        refs = refs[count:]
        total = keep[0].astype(F32) + received[0].astype(F32)
        for other in others:
            total = total + other[...].astype(F32)
        out_ref[h * blocks : (h + 1) * blocks] = total.astype(BF).reshape(blocks, cap, width)
        for step in range(h * blocks, (h + 1) * blocks):
            copies.append(
                pltpu.make_async_copy(out_ref.at[step], out_hbm.at[me ^ step], sems.at[step])
            )
            copies[-1].start()
    wait(copies)


def finish(groups, shape):
    return small_call(
        functools.partial(finish_kernel, [len(g) for g in groups]),
        [a for g in groups for a in g],
        [pltpu.HBM(shape, BF)],
        [pltpu.VMEM(shape, BF), pltpu.SemaphoreType.DMA((shape[0],))],
    )[0]


def total_kernel(keep_ref, received_ref, *refs):
    others, out_ref = refs[:-1], refs[-1]
    total = keep_ref[0].astype(F32) + received_ref[0].astype(F32)
    for other in others:
        total = total + other[...].astype(F32)
    out_ref[...] = total


def add_all(keep, received, others):
    shape = jax.ShapeDtypeStruct(keep.shape[1:], F32)
    return small_call(total_kernel, [keep, received, *others], [shape])[0]


def combine_kernel(top, plan_hbm, slots_ref, shared_ref, out_ref, plan_ref, sems):
    copies = fetch([plan_hbm], [plan_ref], sems)
    rows = plan_ref.shape[0]
    experts, cap, width = slots_ref.shape
    n = lax.broadcasted_iota(jnp.int32, (rows, experts * cap), 1)
    total = shared_ref[...]
    wait(copies)
    for k in range(top):
        pick = jnp.where(n == plan_ref[:, k : k + 1].astype(jnp.int32), 1.0, 0.0).astype(BF)
        picked = dot(pick, slots_ref[...].reshape(experts * cap, width))
        total = total + picked * plan_ref[:, top + k : top + k + 1]
    out_ref[...] = total.astype(BF)


def combine(plan, top, slots, shared):
    rows = plan.shape[0]
    args = (slots, shared)
    return pl.pallas_call(
        functools.partial(combine_kernel, top),
        in_specs=[HBM] + [VMEM] * len(args),
        out_specs=VMEM,
        out_shape=jax.ShapeDtypeStruct((rows, slots.shape[2]), BF),
        scratch_shapes=room([plan]),
        compiler_params=params(16),
        cost_estimate=cost(8e8, 2e6),
        name="combine",
    )(*in_hbm([plan]), *args)


def core_swap(x):
    n = lax.axis_size("tp")
    return lax.ppermute(x, "tp", [(i, i ^ 1) for i in range(n)])


def chip_shift(x, step):
    n = lax.axis_size("tp")
    return lax.ppermute(x, "tp", [(i, (i + 2 * step) % n) for i in range(n)])


def gather_lanes(x, halves):
    mine = [x] + [chip_shift(x, s) for s in range(1, halves)]
    other = [core_swap(m) for m in mine]
    offsets = [(s, 0) for s in range(halves)] + [(s, 1) for s in range(halves)]
    return mine + other, offsets


def scatter_chips(keep, received):
    terms = add_terms(keep, received)
    return [chip_shift(t, s + 1) for s, t in enumerate(terms)]


def ep_gather(x, axis_z, axis_x):
    n = lax.axis_size("ep")
    own = [x]
    for step in range(1, axis_z):
        own.append(lax.ppermute(x, "ep", [(i, (i + step * axis_x) % n) for i in range(n)]))
    stacked = stack(own)
    groups = [stacked]
    for step in range(1, axis_x):
        perm = [(i, i // axis_x * axis_x + (i + step) % axis_x) for i in range(n)]
        groups.append(lax.ppermute(stacked, "ep", perm))
    return groups


def exchange(x):
    return lax.all_to_all(x, "ep", 0, 0, tiled=True)


def body(
    x_size,
    query_rows,
    key_rows,
    value_rows,
    query_gain,
    key_gain,
    out_weight,
    mixer_gain,
    expert_input,
    expert_ids,
    gate_score,
    expert_gain,
    gate_weight,
    up_weight,
    down_weight,
    shared_gate,
    shared_up,
    shared_down,
):
    return whole_step(
        x_size,
        query_rows,
        key_rows,
        value_rows,
        query_gain,
        key_gain,
        out_weight,
        mixer_gain,
        expert_input,
        expert_ids,
        gate_score,
        expert_gain,
        gate_weight,
        up_weight,
        down_weight,
        shared_gate,
        shared_up,
        shared_down,
    )


def whole_step(
    x_size,
    query_rows,
    key_rows,
    value_rows,
    query_gain,
    key_gain,
    out_weight,
    mixer_gain,
    expert_input,
    expert_ids,
    gate_score,
    expert_gain,
    gate_weight,
    up_weight,
    down_weight,
    shared_gate,
    shared_up,
    shared_down,
):
    ep, tp = lax.axis_size("ep"), lax.axis_size("tp")
    halves = tp // 2
    heads = query_rows.shape[1] // HEAD_DIM
    assert tp > 2 and tp % 2 == 0 and heads <= HEADS // KV_HEADS and gate_weight.shape[0] == 1
    rows, top = expert_ids.shape
    width = expert_input.shape[1] // tp
    cap = 3 * rows * top // (2 * ep)
    chunks = 2
    size = ep * cap // chunks

    eighth = out_weight.shape[0] // 8
    ends = (0, 4 * eighth, 8 * eighth)
    parts = [out_weight[i:j] for i, j in zip(ends, ends[1:])]
    w_list = [[out_weight]]
    for step in range(1, halves):
        w_list.append([chip_shift(w, step) for w in parts])
    w_list += [[core_swap(w) for w in parts] for parts in w_list]

    normed, plan, *outgoing = route(
        expert_ids, gate_score, expert_input, expert_gain, ep, cap, width
    )
    blocks = [outgoing[0]]
    for step in range(1, ep):
        blocks.append(lax.ppermute(outgoing[step], "ep", [(i, i ^ step) for i in range(ep)]))
    part = ep // chunks
    arrived = [stack(blocks[h * part : (h + 1) * part]).reshape(size, width) for h in range(chunks)]

    shared = (shared_gate[None], shared_up[None], shared_down[None])
    sh_send, sh_keep = mlp([normed], [None], shared, halves)
    sh_received = core_swap(sh_send)
    sh_others = scatter_chips(sh_keep, sh_received)

    weights = [gate_weight, up_weight, down_weight]
    own_chip = [p for x in arrived for p in (x, core_swap(x))]
    (partial,) = mlp(own_chip, [(0, 0), (0, 1)], weights, halves, True)
    results = []
    for h, x in enumerate(arrived):
        mine = [chip_shift(x, s) for s in range(1, halves)]
        other = [core_swap(m) for m in mine]
        offsets = [(s, c) for c in range(2) for s in range(1, halves)]
        send, keep = mlp(mine + other, offsets, weights, halves, partial=partial, chunk=h)
        received = core_swap(send)
        results.append((keep, received, *scatter_chips(keep, received)))
    returned = exchange(finish(results, (ep, cap, width)))
    shared_sum = add_all(sh_keep, sh_received, sh_others)
    expert_out = combine(plan, top, returned, shared_sum)

    kv, table = prepare_keys(key_rows, value_rows, key_gain, heads)
    kv_list = ep_gather(kv, ep // x_size, x_size)
    attended = attention(query_rows, kv_list, query_gain, table)[:, : query_rows.shape[1]]
    att_list, _ = gather_lanes(attended, halves)
    mixer_out = project(att_list, w_list, mixer_gain)
    return (mixer_out, expert_out)


def solution(mesh):
    in_specs = (
        P("ep", "tp"),
        P("ep", None),
        P("ep", None),
        P(),
        P(),
        P("tp", None),
        P(),
        P("ep", None),
        P("ep", None),
        P("ep", None),
        P(),
        P("ep", None, "tp"),
        P("ep", None, "tp"),
        P("ep", "tp", None),
        P(None, "tp"),
        P(None, "tp"),
        P("tp", None),
    )
    out_specs = (P("ep", None), P("ep", "tp"))
    ep = mesh.shape["ep"]
    x_size = 2 ** (int(math.log2(ep)) // 2)
    return jax.shard_map(
        functools.partial(body, x_size),
        mesh=mesh,
        in_specs=in_specs,
        out_specs=out_specs,
        check_vma=False,
    )
```

```python
import functools
import math

import jax
import jax.numpy as jnp
import numpy as np
from jax import lax
from jax.experimental import pallas as pl
from jax.experimental.pallas import tpu as pltpu
from jax.sharding import PartitionSpec as P


HEADS = 16
KV_HEADS = 4
HEAD_DIM = 64
GRID_W = 64
EPSILON = 1e-06
ROUTED_SCALE = 2.5
LOG2E = 1.4426950408889634
BF = jnp.bfloat16
F32 = jnp.float32
VMEM = pl.BlockSpec(memory_space=pltpu.VMEM)
HBM = pl.BlockSpec(memory_space=pltpu.HBM)


def params(mib):
    return pltpu.CompilerParams(vmem_limit_bytes=mib * 1024 * 1024)


def cost(flops, bytes_accessed, exps=0):
    return pl.CostEstimate(
        flops=int(flops), bytes_accessed=int(bytes_accessed), transcendentals=int(exps)
    )


def in_hbm(arrays):
    return [pltpu.with_memory_space_constraint(a, pltpu.HBM) for a in arrays]


def fetch(sources, targets, sems):
    copies = [
        pltpu.make_async_copy(a, b, sems.at[i]) for i, (a, b) in enumerate(zip(sources, targets))
    ]
    for copy in copies:
        copy.start()
    return copies


def wait(copies):
    for copy in copies:
        copy.wait()


def room(arrays):
    return [pltpu.VMEM(a.shape, a.dtype) for a in arrays] + [
        pltpu.SemaphoreType.DMA((len(arrays),))
    ]


def dot(a, b, dims=((1,), (0,))):
    return lax.dot_general(a, b, (dims, ((), ())), preferred_element_type=F32)


def rotate_block(x, gain, table_ref, grid_rows, g):
    lane = lax.broadcasted_iota(jnp.int32, x.shape, 1)
    squares = x * x
    first = lane < HEAD_DIM
    sum_a = jnp.sum(jnp.where(first, squares, 0.0), axis=1, keepdims=True)
    sum_b = jnp.sum(jnp.where(first, 0.0, squares), axis=1, keepdims=True)
    mean = jnp.where(first, sum_a, sum_b) * (1.0 / HEAD_DIM)
    y = x * lax.rsqrt(mean + EPSILON) * gain
    by_row = lane % 32 < 16
    height = grid_rows + GRID_W
    cosine = jnp.where(by_row, table_ref[g : g + 1, :], table_ref[grid_rows:height, :])
    sine = jnp.where(
        by_row,
        table_ref[height + g : height + g + 1, :],
        table_ref[height + grid_rows : 2 * height, :],
    )
    swapped = jnp.where(lane % HEAD_DIM < 32, pltpu.roll(y, 96, 1), pltpu.roll(y, 32, 1))
    return y * cosine + swapped * sine


def key_kernel(
    heads, key_hbm, value_hbm, gain_hbm, inverse_hbm, out_ref, table_ref, key_ref, value_ref,
    gain_ref, inverse_ref, sems,
):
    kv_index = lax.axis_index("tp") * heads * KV_HEADS // HEADS
    cols = pl.ds(pl.multiple_of(kv_index // 2 * 128, 128), 128)
    copies = fetch(
        [inverse_hbm, gain_hbm, key_hbm.at[:, cols], value_hbm.at[:, cols]],
        [inverse_ref, gain_ref, key_ref, value_ref],
        sems,
    )
    wait(copies[:1])
    local_rows = key_ref.shape[0]
    grid_rows = local_rows // GRID_W
    height = grid_rows + GRID_W
    index = lax.broadcasted_iota(jnp.int32, (height, 128), 0)
    place = jnp.where(
        index < grid_rows, lax.axis_index("ep") * grid_rows + index, index - grid_rows
    )
    angle = place.astype(F32) * inverse_ref[...]
    lanes = lax.broadcasted_iota(jnp.int32, (height, 128), 1)
    table_ref[:height, :] = jnp.cos(angle)
    sine = jnp.sin(angle)
    table_ref[height:, :] = jnp.where(lanes % HEAD_DIM < HEAD_DIM // 2, -sine, sine)
    odd = kv_index % 2 == 1
    wait(copies[1:])
    gain = jnp.concatenate([gain_ref[...]] * 2, axis=1)
    lane = lax.broadcasted_iota(jnp.int32, (GRID_W, 128), 1)
    for g in range(grid_rows):
        rows = slice(g * GRID_W, (g + 1) * GRID_W)
        keys = key_ref[rows, :].astype(F32)
        values = value_ref[rows, :].astype(F32)
        turned = rotate_block(keys, gain, table_ref, grid_rows, g)
        turned = jnp.where(odd, pltpu.roll(turned, 64, 1), turned)
        values = jnp.where(odd, values, pltpu.roll(values, 64, 1))
        out_ref[rows, :] = jnp.where(lane < HEAD_DIM, turned, values).astype(BF)


def prepare_keys(key_rows, value_rows, gain, heads):
    local_rows = key_rows.shape[0]
    height = local_rows // GRID_W + GRID_W
    quarter = HEAD_DIM // 4
    inverse = 10000.0 ** (-np.arange(quarter, dtype=np.float32) / quarter)
    inverse = jnp.asarray(np.tile(inverse, 128 // quarter)[None, :], F32)
    args = (key_rows, value_rows, gain[None, :], inverse)
    return pl.pallas_call(
        functools.partial(key_kernel, heads),
        in_specs=[HBM] * 4,
        out_specs=[VMEM] * 2,
        out_shape=[
            jax.ShapeDtypeStruct((local_rows, 128), BF),
            jax.ShapeDtypeStruct((2 * height, 128), F32),
        ],
        scratch_shapes=[pltpu.VMEM((local_rows, 128), BF)] * 2 + room(args[2:])[:2]
        + [pltpu.SemaphoreType.DMA((4,))],
        compiler_params=params(8),
        cost_estimate=cost(1e9, 3e5),
        name="keys",
    )(*in_hbm(args))


def attention_kernel(heads, tile, chunk, n_kv, q_hbm, gain_hbm, table_hbm, *rest):
    kv_refs = rest[:n_kv]
    att_ref, qs_ref, sa_ref, sb_ref, o_ref, kt_ref, q_ref, gain_ref, table_ref, sems = rest[n_kv:]
    copies = fetch([q_hbm, gain_hbm, table_hbm], [q_ref, gain_ref, table_ref], sems)
    local_rows = q_ref.shape[0]
    grid_rows = local_rows // GRID_W
    blocks = [ref.at[b] for ref in kv_refs for b in range(ref.shape[0])]
    for i, ref in enumerate(blocks):
        kt_ref[:, i * local_rows : (i + 1) * local_rows] = ref[...].astype(F32).T.astype(BF)
    keys = len(blocks) * local_rows
    wait(copies)
    lane = lax.broadcasted_iota(jnp.int32, (GRID_W, 128), 1)
    gain = jnp.concatenate([gain_ref[...]] * 2, axis=1)
    pairs = q_ref.shape[1] // 128
    for pair in range(pairs):
        for g in range(grid_rows):
            x = q_ref[g * GRID_W : (g + 1) * GRID_W, pair * 128 : (pair + 1) * 128].astype(F32)
            turned = rotate_block(x, gain, table_ref, grid_rows, g)
            turned = turned.astype(BF).astype(F32) * HEAD_DIM ** (-0.5)
            for k in range(min(2, heads - 2 * pair)):
                own = turned if k == 0 else pltpu.roll(turned, 64, 1)
                start = (2 * pair + k) * local_rows + g * GRID_W
                qs_ref[start : start + GRID_W, :] = jnp.where(lane < HEAD_DIM, own, 0.0).astype(BF)

    def score(q, s_ref, at, peak):
        s = dot(q, kt_ref[:, at : at + chunk]) * LOG2E
        s_ref[:, at : at + chunk] = s
        for c in range(0, chunk, 128):
            part = s[:, c : c + 128]
            peak = part if peak is None else jnp.maximum(peak, part)
        return peak

    tiles = heads * local_rows // tile
    buffers = (sa_ref, sb_ref)
    peak = None
    for at in range(0, keys, chunk):
        peak = score(qs_ref[:tile, :], sa_ref, at, peak)
    peak = jnp.max(peak, axis=1, keepdims=True)
    for i in range(tiles):
        begin = i * tile
        total = jnp.zeros((tile, 128), F32)
        accum = jnp.zeros((tile, 128), F32)
        next_peak = None
        for at in range(0, keys, chunk):
            if i + 1 < tiles:
                q = qs_ref[begin + tile : begin + 2 * tile, :]
                next_peak = score(q, buffers[(i + 1) % 2], at, next_peak)
            e = jnp.exp2(buffers[i % 2][:, at : at + chunk] - peak)
            for c in range(0, chunk, 128):
                total = total + e[:, c : c + 128]
            e = e.astype(BF)
            for c in range(0, chunk, local_rows):
                accum = accum + dot(e[:, c : c + local_rows], blocks[(at + c) // local_rows][...])
        o_ref[begin : begin + tile, :] = accum / jnp.sum(total, axis=1, keepdims=True)
        if i + 1 < tiles:
            peak = jnp.max(next_peak, axis=1, keepdims=True)
    wide = lax.broadcasted_iota(jnp.int32, (local_rows, 128), 1)
    for pair in range(pairs):
        start = 2 * pair * local_rows
        low = pltpu.roll(o_ref[start : start + local_rows, :], 64, 1)
        if heads > 2 * pair + 1:
            high = o_ref[start + local_rows : start + 2 * local_rows, :]
        else:
            high = jnp.zeros((local_rows, 128), F32)
        att_ref[:, pair * 128 : (pair + 1) * 128] = jnp.where(wide < HEAD_DIM, low, high).astype(BF)


def attention(query_rows, kv_list, gain, table):
    local_rows, width = query_rows.shape
    heads = width // HEAD_DIM
    if width % 128:
        query_rows = jnp.pad(query_rows, ((0, 0), (0, 64)))
    keys = sum(k.shape[0] * k.shape[1] for k in kv_list)
    chunk = 2 * local_rows if keys % (2 * local_rows) == 0 else local_rows
    tile = 256 if heads * local_rows % 256 == 0 else 128
    args = (query_rows, gain[None, :], table)
    attended = pl.pallas_call(
        functools.partial(attention_kernel, heads, tile, chunk, len(kv_list)),
        in_specs=[HBM] * 3 + [VMEM] * len(kv_list),
        out_specs=VMEM,
        out_shape=jax.ShapeDtypeStruct(query_rows.shape, BF),
        scratch_shapes=[
            pltpu.VMEM((heads * local_rows, 128), BF),
            pltpu.VMEM((tile, keys), F32),
            pltpu.VMEM((tile, keys), F32),
            pltpu.VMEM((heads * local_rows, 128), F32),
            pltpu.VMEM((128, keys), BF),
        ]
        + room(args),
        compiler_params=params(24),
        cost_estimate=cost(8e9, 2e6, heads * local_rows * keys),
        name="attention",
    )(*in_hbm(args), *kv_list)
    return attended[:, :width]


def project_kernel(counts, block, *refs):
    att_refs, rest = refs[: len(counts)], refs[len(counts) :]
    w_refs = []
    for count in counts:
        w_refs.append(rest[:count])
        rest = rest[count:]
    gain_ref, out_ref, sum_ref = rest
    rows, model = out_ref.shape
    squares = jnp.zeros((rows, 128), F32)
    for at in range(0, model, block):
        total = None
        for a, parts in zip(att_refs, w_refs):
            part, row = None, 0
            for w in parts:
                term = dot(a[:, row : row + w.shape[0]], w[:, at : at + block])
                part = term if part is None else part + term
                row += w.shape[0]
            part = part.astype(BF).astype(F32)
            total = part if total is None else total + part
        sum_ref[:, at : at + block] = total
        for c in range(0, block, 128):
            squares = squares + total[:, c : c + 128] * total[:, c : c + 128]
    mean = jnp.sum(squares, axis=1, keepdims=True) * (1.0 / model)
    scale = lax.rsqrt(mean + EPSILON)
    for at in range(0, model, block):
        cols = slice(at, at + block)
        out_ref[:, cols] = (sum_ref[:, cols] * scale * gain_ref[:, cols]).astype(BF)


def project(att_list, w_list, gain):
    rows, model = att_list[0].shape[0], w_list[0][0].shape[1]
    args = (*att_list, *(w for parts in w_list for w in parts), gain[None, :])
    return pl.pallas_call(
        functools.partial(project_kernel, [len(w) for w in w_list], min(256, model)),
        in_specs=[VMEM] * len(args),
        out_specs=VMEM,
        out_shape=jax.ShapeDtypeStruct((rows, model), BF),
        scratch_shapes=[pltpu.VMEM((rows, model), F32)],
        compiler_params=params(32),
        cost_estimate=cost(2e9, 6e6),
        name="project",
    )(*args)


def route_kernel(
    experts, cap, ids_hbm, score_hbm, x_hbm, gain_hbm, normed_ref, plan_hbm, *refs
):
    out_refs = refs[:experts]
    plan_ref, place_ref, idst_ref, score_ref, x_ref, gain_ref, sems, out_sem = refs[experts:]
    copies = fetch(
        [ids_hbm, score_hbm, gain_hbm, x_hbm], [idst_ref, score_ref, gain_ref, x_ref], sems
    )
    wait(copies[:2])
    top, rows = idst_ref.shape
    names = lax.broadcasted_iota(jnp.int32, (experts, rows), 0)
    hits = [idst_ref[k : k + 1, :] == names for k in range(top)]
    named = functools.reduce(jnp.logical_or, hits)
    r0 = lax.broadcasted_iota(jnp.int32, (rows, rows), 0)
    r1 = lax.broadcasted_iota(jnp.int32, (rows, rows), 1)
    above = jnp.where(r0 < r1, 1.0, 0.0).astype(BF)
    count = dot(jnp.where(named, 1.0, 0.0).astype(BF), above)
    scores = [score_ref[k : k + 1, :] for k in range(top)]
    score_sum = functools.reduce(jnp.add, scores)
    lines = []
    for k in range(top):
        rank = jnp.sum(jnp.where(hits[k], count, 0.0), axis=0, keepdims=True)
        lines.append((idst_ref[k : k + 1, :] * cap).astype(F32) + rank)
    lines += [s / score_sum * ROUTED_SCALE for s in scores]
    lines += [jnp.zeros((8 - 2 * top, rows), F32)]
    plan_ref[...] = jnp.concatenate(lines, axis=0).T
    sent = pltpu.make_async_copy(plan_ref, plan_hbm, out_sem)
    sent.start()
    place_ref[...] = jnp.where(named, count.astype(jnp.int32), -1)
    wait(copies[2:])
    x = x_ref[...].astype(F32)
    mean = jnp.mean(x * x, axis=1, keepdims=True)
    normed_ref[...] = (x * lax.rsqrt(mean + EPSILON) * gain_ref[...]).astype(BF)
    width = out_refs[0].shape[1]
    own = normed_ref[:, pl.ds(pl.multiple_of(lax.axis_index("tp") * width, 128), width)]
    slots = lax.broadcasted_iota(jnp.int32, (cap, rows), 0)
    me = lax.axis_index("ep")
    for step, ref in enumerate(out_refs):
        place = place_ref[pl.ds(me ^ step, 1), :]
        ref[...] = dot(jnp.where(place == slots, 1.0, 0.0).astype(BF), own).astype(BF)
    sent.wait()


def route(expert_ids, gate_score, expert_input, gain, experts, cap, width):
    rows = expert_ids.shape[0]
    args = (expert_ids.T, gate_score.T, expert_input, gain[None, :])
    normed = jax.ShapeDtypeStruct(expert_input.shape, BF)
    block = jax.ShapeDtypeStruct((cap, width), BF)
    return pl.pallas_call(
        functools.partial(route_kernel, experts, cap),
        in_specs=[HBM] * 4,
        out_specs=[VMEM, HBM] + [VMEM] * experts,
        out_shape=[normed, pltpu.HBM((rows, 8), F32)] + [block] * experts,
        scratch_shapes=[pltpu.VMEM((rows, 8), F32), pltpu.VMEM((experts, rows), jnp.int32)]
        + room(args)
        + [pltpu.SemaphoreType.DMA],
        compiler_params=params(16),
        cost_estimate=cost(1e9, 4e6),
        name="route",
    )(*in_hbm(args))


def loads_of(hidden):
    return 2 if hidden % 512 == 0 else 1


def mlp_kernel(n_x, halves, offsets, early, late, chunk, *refs):
    x_refs, refs = refs[:n_x], refs[n_x:]
    if late:
        partial_ref, refs = refs[0], refs[1:]
    gate_hbm, up_hbm, refs = refs[0], refs[1], refs[2:]
    if early:
        out_ref, gate_ref, up_ref, sems = refs
    else:
        down_hbm, send_ref, keep_ref, gate_ref, up_ref, sems, h_ref, down_ref = refs
    lane = lax.axis_index("tp")
    chip, side = lane // 2, lane % 2
    hidden = gate_ref.shape[1]
    block = min(256, hidden // loads_of(hidden))
    rows, row = [], 0
    for ref, offset in zip(x_refs, offsets):
        size = ref.shape[1]
        begin = 0
        if offset is not None:
            source = 2 * lax.rem(chip + halves - offset[0], halves)
            source = source + (side if offset[1] == 0 else 1 - side)
            begin = pl.multiple_of(source * size, 128)
        rows.append((pl.ds(begin, size), slice(row, row + size)))
        row += size
    loads = loads_of(hidden)
    load = hidden // loads
    groups = []
    for at in range(0, hidden, load):
        cols = slice(at, at + load)
        groups.append(
            [
                (w_hbm.at[0, there, cols], w_ref.at[here, cols])
                for w_hbm, w_ref in ((gate_hbm, gate_ref), (up_hbm, up_ref))
                for there, here in rows
            ]
        )
    if not early:
        width = send_ref.shape[2]
        goals = [(1 - side, step, send_ref) for step in range(halves)]
        goals += [(side, step, keep_ref) for step in range(halves)]
        groups.append([])
        for i, (core, step, unused) in enumerate(goals):
            goal = 2 * lax.rem(chip + step, halves) + core
            begin = pl.multiple_of(goal * width, 128)
            groups[-1].append((down_hbm.at[0, :, pl.ds(begin, width)], down_ref.at[i]))
    number = 0
    for i, group in enumerate(groups):
        groups[i] = [
            pltpu.make_async_copy(x, y, sems.at[number + j]) for j, (x, y) in enumerate(group)
        ]
        number += len(group)

    def start(i):
        for copy in groups[i] if i < len(groups) else ():
            copy.start()

    start(0)
    if loads > 1:
        start(1)

    def product(w_ref, cols, x_refs):
        total = None
        for ref, (unused, here) in zip(x_refs, rows):
            term = dot(ref[...], w_ref[here, cols])
            total = term if total is None else total + term
        return total

    for at in range(0, hidden, block):
        cols = slice(at, at + block)
        if at % load == 0:
            wait(groups[at // load])
            start(at // load + min(2, loads))
        for h in range(0, n_x, len(offsets)):
            gate = product(gate_ref, cols, x_refs[h : h + len(offsets)])
            up = product(up_ref, cols, x_refs[h : h + len(offsets)])
            if early:
                taken = slice(h // len(offsets) * gate.shape[0], (h // len(offsets) + 1) * gate.shape[0])
                out_ref[0, taken, cols] = gate
                out_ref[1, taken, cols] = up
                continue
            if late:
                taken = slice(chunk * gate.shape[0], (chunk + 1) * gate.shape[0])
                gate = gate + partial_ref[0, taken, cols]
                up = up + partial_ref[1, taken, cols]
            h_ref[:, cols] = (gate / (1.0 + jnp.exp(-gate)) * up).astype(BF)
    if early:
        return
    inner = min(256, width)
    wait(groups[-1])
    for i, (unused, step, out) in enumerate(goals):
        for at in range(0, width, inner):
            cols = slice(at, at + inner)
            out[step, :, cols] = dot(h_ref[...], down_ref[i, :, cols]).astype(BF)


def mlp(x_list, offsets, weights, halves, early=False, partial=None, chunk=0):
    rows = x_list[0].shape[0]
    model, hidden = weights[0].shape[1:]
    width = model // (2 * halves)
    depth = sum(x.shape[1] for x in x_list[: len(offsets)])
    n_copies = 2 * len(offsets) * loads_of(hidden)
    if early:
        weights = weights[:2]
        outs = [jax.ShapeDtypeStruct((2, len(x_list) // len(offsets) * rows, hidden), F32)]
    else:
        n_copies += 2 * halves
        outs = [jax.ShapeDtypeStruct((halves, rows, width), BF)] * 2
    scratch = [pltpu.VMEM((depth, hidden), BF)] * 2 + [pltpu.SemaphoreType.DMA((n_copies,))]
    if not early:
        scratch += [pltpu.VMEM((rows, hidden), BF), pltpu.VMEM((2 * halves, hidden, width), BF)]
    late = [] if partial is None else [partial]
    flops = 4 * rows * depth * hidden + (0 if early else 2 * rows * model * hidden)
    return pl.pallas_call(
        functools.partial(mlp_kernel, len(x_list), halves, offsets, early, bool(late), chunk),
        in_specs=[VMEM] * len(x_list + late) + [HBM] * len(weights),
        out_specs=[VMEM] * len(outs),
        out_shape=outs,
        scratch_shapes=scratch,
        compiler_params=params(24),
        cost_estimate=cost(flops, 6 * model * hidden),
    )(*x_list, *late, *in_hbm(weights))


def small_call(kernel, args, outs, scratch=()):
    return pl.pallas_call(
        kernel,
        in_specs=[VMEM] * len(args),
        out_specs=[HBM if isinstance(o, type(pltpu.HBM((8, 128), F32))) else VMEM for o in outs],
        out_shape=outs,
        scratch_shapes=list(scratch),
        compiler_params=params(4),
        cost_estimate=cost(1e8, 2e6),
    )(*args)


def stack_kernel(*refs):
    for i, ref in enumerate(refs[:-1]):
        refs[-1][i] = ref[...]


def stack(arrays):
    shape = jax.ShapeDtypeStruct((len(arrays), *arrays[0].shape), arrays[0].dtype)
    return small_call(stack_kernel, arrays, [shape])[0]


def add_kernel(a_ref, b_ref, *outs):
    for i, out in enumerate(outs):
        out[...] = (a_ref[1 + i].astype(F32) + b_ref[1 + i].astype(F32)).astype(BF)


def add_terms(keep, received):
    shape = jax.ShapeDtypeStruct(keep.shape[1:], BF)
    return small_call(add_kernel, [keep, received], [shape] * (keep.shape[0] - 1))


def finish_kernel(counts, *refs):
    refs, out_hbm, out_ref, sems = refs[:-3], refs[-3], refs[-2], refs[-1]
    ep, cap, width = out_ref.shape
    blocks = ep // len(counts)
    me = lax.axis_index("ep")
    copies = []
    for h, count in enumerate(counts):
        keep, received, others = refs[0], refs[1], refs[2:count]
        refs = refs[count:]
        total = keep[0].astype(F32) + received[0].astype(F32)
        for other in others:
            total = total + other[...].astype(F32)
        out_ref[h * blocks : (h + 1) * blocks] = total.astype(BF).reshape(blocks, cap, width)
        for step in range(h * blocks, (h + 1) * blocks):
            copies.append(
                pltpu.make_async_copy(out_ref.at[step], out_hbm.at[me ^ step], sems.at[step])
            )
            copies[-1].start()
    wait(copies)


def finish(groups, shape):
    return small_call(
        functools.partial(finish_kernel, [len(g) for g in groups]),
        [a for g in groups for a in g],
        [pltpu.HBM(shape, BF)],
        [pltpu.VMEM(shape, BF), pltpu.SemaphoreType.DMA((shape[0],))],
    )[0]


def total_kernel(plan_ref, keep_ref, received_ref, *refs):
    others, (out_ref, kept_ref) = refs[:-2], refs[-2:]
    kept_ref[...] = plan_ref[...]
    total = keep_ref[0].astype(F32) + received_ref[0].astype(F32)
    for other in others:
        total = total + other[...].astype(F32)
    out_ref[...] = total


def add_all(plan, keep, received, others):
    outs = [jax.ShapeDtypeStruct(keep.shape[1:], F32), jax.ShapeDtypeStruct(plan.shape, F32)]
    return small_call(total_kernel, [plan, keep, received, *others], outs)


def combine_kernel(top, plan_ref, slots_ref, shared_ref, out_ref):
    rows = plan_ref.shape[0]
    experts, cap, width = slots_ref.shape
    n = lax.broadcasted_iota(jnp.int32, (rows, experts * cap), 1)
    total = shared_ref[...]
    for k in range(top):
        pick = jnp.where(n == plan_ref[:, k : k + 1].astype(jnp.int32), 1.0, 0.0).astype(BF)
        picked = dot(pick, slots_ref[...].reshape(experts * cap, width))
        total = total + picked * plan_ref[:, top + k : top + k + 1]
    out_ref[...] = total.astype(BF)


def combine(plan, top, slots, shared):
    rows = plan.shape[0]
    args = (plan, slots, shared)
    return pl.pallas_call(
        functools.partial(combine_kernel, top),
        in_specs=[VMEM] * len(args),
        out_specs=VMEM,
        out_shape=jax.ShapeDtypeStruct((rows, slots.shape[2]), BF),
        compiler_params=params(16),
        cost_estimate=cost(8e8, 2e6),
        name="combine",
    )(*args)


def core_swap(x):
    n = lax.axis_size("tp")
    return lax.ppermute(x, "tp", [(i, i ^ 1) for i in range(n)])


def chip_shift(x, step):
    n = lax.axis_size("tp")
    return lax.ppermute(x, "tp", [(i, (i + 2 * step) % n) for i in range(n)])


def gather_lanes(x, halves):
    mine = [x] + [chip_shift(x, s) for s in range(1, halves)]
    other = [core_swap(m) for m in mine]
    offsets = [(s, 0) for s in range(halves)] + [(s, 1) for s in range(halves)]
    return mine + other, offsets


def scatter_chips(keep, received):
    terms = add_terms(keep, received)
    return [chip_shift(t, s + 1) for s, t in enumerate(terms)]


def ep_gather(x, axis_z, axis_x):
    n = lax.axis_size("ep")
    own = [x]
    for step in range(1, axis_z):
        own.append(lax.ppermute(x, "ep", [(i, (i + step * axis_x) % n) for i in range(n)]))
    stacked = stack(own)
    groups = [stacked]
    for step in range(1, axis_x):
        perm = [(i, i // axis_x * axis_x + (i + step) % axis_x) for i in range(n)]
        groups.append(lax.ppermute(stacked, "ep", perm))
    return groups


def exchange(x):
    return lax.all_to_all(x, "ep", 0, 0, tiled=True)


def body(
    x_size,
    query_rows,
    key_rows,
    value_rows,
    query_gain,
    key_gain,
    out_weight,
    mixer_gain,
    expert_input,
    expert_ids,
    gate_score,
    expert_gain,
    gate_weight,
    up_weight,
    down_weight,
    shared_gate,
    shared_up,
    shared_down,
):
    return whole_step(
        x_size,
        query_rows,
        key_rows,
        value_rows,
        query_gain,
        key_gain,
        out_weight,
        mixer_gain,
        expert_input,
        expert_ids,
        gate_score,
        expert_gain,
        gate_weight,
        up_weight,
        down_weight,
        shared_gate,
        shared_up,
        shared_down,
    )


def whole_step(
    x_size,
    query_rows,
    key_rows,
    value_rows,
    query_gain,
    key_gain,
    out_weight,
    mixer_gain,
    expert_input,
    expert_ids,
    gate_score,
    expert_gain,
    gate_weight,
    up_weight,
    down_weight,
    shared_gate,
    shared_up,
    shared_down,
):
    ep, tp = lax.axis_size("ep"), lax.axis_size("tp")
    halves = tp // 2
    heads = query_rows.shape[1] // HEAD_DIM
    assert tp > 2 and tp % 2 == 0 and heads <= HEADS // KV_HEADS and gate_weight.shape[0] == 1
    rows, top = expert_ids.shape
    width = expert_input.shape[1] // tp
    cap = 3 * rows * top // (2 * ep)
    chunks = 2
    size = ep * cap // chunks

    eighth = out_weight.shape[0] // 8
    ends = (0, 5 * eighth, 8 * eighth)
    parts = [out_weight[i:j] for i, j in zip(ends, ends[1:])]
    w_list = [[out_weight]]
    for step in range(1, halves):
        w_list.append([chip_shift(w, step) for w in parts])
    w_list += [[core_swap(w) for w in parts] for parts in w_list]

    normed, plan, *outgoing = route(
        expert_ids, gate_score, expert_input, expert_gain, ep, cap, width
    )
    blocks = [outgoing[0]]
    for step in range(1, ep):
        blocks.append(lax.ppermute(outgoing[step], "ep", [(i, i ^ step) for i in range(ep)]))
    part = ep // chunks
    arrived = [stack(blocks[h * part : (h + 1) * part]).reshape(size, width) for h in range(chunks)]

    shared = (shared_gate[None], shared_up[None], shared_down[None])
    sh_send, sh_keep = mlp([normed], [None], shared, halves)
    sh_received = core_swap(sh_send)
    sh_others = scatter_chips(sh_keep, sh_received)

    weights = [gate_weight, up_weight, down_weight]
    own_chip = [p for x in arrived for p in (x, core_swap(x))]
    (partial,) = mlp(own_chip, [(0, 0), (0, 1)], weights, halves, True)
    results = []
    for h, x in enumerate(arrived):
        mine = [chip_shift(x, s) for s in range(1, halves)]
        other = [core_swap(m) for m in mine]
        offsets = [(s, c) for c in range(2) for s in range(1, halves)]
        send, keep = mlp(mine + other, offsets, weights, halves, partial=partial, chunk=h)
        received = core_swap(send)
        results.append((keep, received, *scatter_chips(keep, received)))
    returned = exchange(finish(results, (ep, cap, width)))
    shared_sum, plan = add_all(plan, sh_keep, sh_received, sh_others)
    expert_out = combine(plan, top, returned, shared_sum)

    kv, table = prepare_keys(key_rows, value_rows, key_gain, heads)
    kv_list = ep_gather(kv, ep // x_size, x_size)
    attended = attention(query_rows, kv_list, query_gain, table)[:, : query_rows.shape[1]]
    att_list, _ = gather_lanes(attended, halves)
    mixer_out = project(att_list, w_list, mixer_gain)
    return (mixer_out, expert_out)


def solution(mesh):
    in_specs = (
        P("ep", "tp"),
        P("ep", None),
        P("ep", None),
        P(),
        P(),
        P("tp", None),
        P(),
        P("ep", None),
        P("ep", None),
        P("ep", None),
        P(),
        P("ep", None, "tp"),
        P("ep", None, "tp"),
        P("ep", "tp", None),
        P(None, "tp"),
        P(None, "tp"),
        P("tp", None),
    )
    out_specs = (P("ep", None), P("ep", "tp"))
    ep = mesh.shape["ep"]
    x_size = 2 ** (int(math.log2(ep)) // 2)
    return jax.shard_map(
        functools.partial(body, x_size),
        mesh=mesh,
        in_specs=in_specs,
        out_specs=out_specs,
        check_vma=False,
    )
```
